128 devices in a mesh: fs: 16 (over z, x), tp: 8 (over y, core).
Axes of the slice: x: 4, y: 4, z: 4, core: 2. Of those that a mesh axis runs over, the one named last changes fastest.
Arguments:
- normed_input: bfloat16 [32768, 2048], P('fs'), may hold values from -6 to 6
- forget_cot: bfloat16 [32768, 2048], P('fs', 'tp'), may hold values from -6 to 6
- value_cot: bfloat16 [32768, 2048], P('fs', 'tp'), may hold values from -6 to 6
- gated_output: bfloat16 [32768, 2048], P('fs', 'tp'), may hold values from -6 to 6
- output_cot: bfloat16 [32768, 2048], P('fs'), may hold values from -6 to 6
- forget_weight: float32 [2048, 2048], P('fs', 'tp'), may hold values from -0.125 to 0.125
- value_weight: float32 [2048, 2048], P('fs', 'tp'), may hold values from -0.125 to 0.125
- out_weight: float32 [2048, 2048], P('tp', 'fs'), may hold values from -0.125 to 0.125
- bases: bfloat16 [3, 2048, 256], replicated, may hold values from -0.125 to 0.125
- first_moment: float32 [256, 3, 2048], P('fs', None, 'tp'), may hold values from -4 to 4
- second_moment: float32 [256, 3, 2048], P('fs', None, 'tp'), may hold values from 0.25 to 4
Outputs:
- new_forget: float32 [2048, 2048], P('fs', 'tp')
- new_value: float32 [2048, 2048], P('fs', 'tp')
- new_out: float32 [2048, 2048], P('tp', 'fs')
- copy_forget: bfloat16 [2048, 2048], P(None, 'tp')
- copy_value: bfloat16 [2048, 2048], P(None, 'tp')
- copy_out: bfloat16 [2048, 2048], P('tp')
- moment_one: float32 [256, 3, 2048], P('fs', None, 'tp')
- moment_two: float32 [256, 3, 2048], P('fs', None, 'tp')
- step_forget: float32 [2048, 2048], P('fs', 'tp')
- step_value: float32 [2048, 2048], P('fs', 'tp')
- step_out: float32 [2048, 2048], P('tp', 'fs')
The draws below stay inside these ranges and needn't reach their ends.
All inputs are finite; a program needn't handle non-finite values.
Results may differ from the reference program's by a relative error of at most 0.0045.
Values may be sent and summed in bfloat16 or wider, within the bound.
A program may use at most 128 MiB of HBM per device.

```python
import math
import jax
import jax.numpy as jnp
from jax import lax

D = 2048
QK = 2048
V = 2048
RANK = 256
TOKENS = 32768


def draw_first_moment(key, part):
    base = jax.random.normal(key, (RANK, 3, QK), jnp.float32) * 0.5
    return jnp.clip(base, -4.0, 4.0)


def level_of(rng, dims, shards, smallest, top_value):
    gain = 1.0
    for dim, shards_of in shards:
        heights = jax.random.uniform(jax.random.fold_in(jax.random.fold_in(rng, 6), dim), (shards_of,), jnp.float32, smallest / len(shards), top_value / len(shards))
        gain = gain * jnp.repeat(jnp.exp(heights), dims[dim] // shards_of).reshape((-1,) + (1,) * (len(dims) - 1 - dim))
    return gain


def normal_values(rng, extent, spread, reach, shards=(), dtype=jnp.bfloat16):
    values = spread * jax.random.normal(rng, extent, jnp.float32)
    if shards:
        values = values * level_of(rng, extent, shards, -0.22, 0.18)
    return jnp.clip(values, -reach, reach).astype(dtype)


def setup_inputs(seed: int = 0) -> dict:
    arg_keys = jax.random.split(jax.random.key(seed), 12)
    normed_input = normal_values(arg_keys[0], (TOKENS, D), 1.0, 6.0, ((0, 16),))
    forget_cot = normal_values(arg_keys[1], (TOKENS, QK), 1.0, 6.0, ((0, 16), (1, 8)))
    value_cot = normal_values(arg_keys[2], (TOKENS, V), 1.0, 6.0, ((0, 16), (1, 8)))
    gated_output = normal_values(arg_keys[3], (TOKENS, V), 1.0, 6.0, ((0, 16), (1, 8)))
    output_cot = normal_values(arg_keys[4], (TOKENS, D), 1.0, 6.0, ((0, 16),))
    forget_weight = normal_values(arg_keys[5], (D, QK), D ** -0.5, 0.125, ((0, 16), (1, 8)), jnp.float32)
    value_weight = normal_values(arg_keys[6], (D, V), D ** -0.5, 0.125, ((0, 16), (1, 8)), jnp.float32)
    out_weight = normal_values(arg_keys[7], (V, D), V ** -0.5, 0.125, ((0, 8), (1, 16)), jnp.float32)
    bases = normal_values(arg_keys[8], (3, D, RANK), D ** -0.5, 0.125)
    first_moment = draw_first_moment(jax.random.fold_in(arg_keys[11], 71), 0)
    second_moment = jnp.clip(jnp.exp(math.log(4.0) - 2.7725887 * jax.random.uniform(arg_keys[10], (RANK, 3, QK), jnp.float32) ** level_of(arg_keys[10], (RANK, 3, QK), ((0, 16), (2, 8)), -0.2, 0.2)), 0.25, 4.0)
    return {"normed_input": normed_input, "forget_cot": forget_cot, "value_cot": value_cot, "gated_output": gated_output, "output_cot": output_cot, "forget_weight": forget_weight, "value_weight": value_weight, "out_weight": out_weight, "bases": bases, "first_moment": first_moment, "second_moment": second_moment}


def reference(normed_input, forget_cot, value_cot, gated_output, output_cot, forget_weight, value_weight, out_weight, bases, first_moment, second_moment):
    factor = float(TOKENS) ** (-0.5)
    grad_forget = jnp.dot(normed_input.T, forget_cot, preferred_element_type=jnp.float32) * factor
    grad_value = jnp.dot(normed_input.T, value_cot, preferred_element_type=jnp.float32) * factor
    grad_out = jnp.dot(output_cot.T, gated_output, preferred_element_type=jnp.float32) * factor
    grads = jnp.stack([grad_forget, grad_value, grad_out], axis=1)
    basis_full = bases.astype(jnp.float32)
    projected = jnp.einsum('kdr,dkc->rkc', basis_full, grads, precision=lax.Precision.HIGHEST)
    moment_one = 0.9 * first_moment + 0.1 * projected
    moment_two = 0.9 * second_moment + 0.1 * projected * projected
    direction = moment_one / (jnp.sqrt(moment_two) + 1e-08)
    scale = lax.rsqrt(lax.optimization_barrier(jnp.mean(direction * direction, axis=(0, 2))) + 1.0)
    full = jnp.einsum('kdr,rkc->dkc', basis_full, direction, precision=lax.Precision.HIGHEST)
    full = full * scale[None, :, None]
    step_forget = full[:, 0, :]
    step_value = full[:, 1, :]
    step_out = full[:, 2, :].T
    new_forget = forget_weight - 0.01 * step_forget
    new_value = value_weight - 0.01 * step_value
    new_out = out_weight - 0.01 * step_out
    return (new_forget, new_value, new_out, new_forget.astype(jnp.bfloat16), new_value.astype(jnp.bfloat16), new_out.astype(jnp.bfloat16), moment_one, moment_two, step_forget, step_value, step_out)
```

```python
import functools

import jax
import jax.numpy as jnp
from jax import lax
from jax.experimental import pallas as pl
from jax.experimental.pallas import tpu as pltpu
from jax.sharding import PartitionSpec as P

MESH = pl.DeviceIdType.MESH
SIDE = 4
STEPS = (1, -1)
OFFSETS = (0, -1, 1, 2)


def exchange_kernel(
    size,
    groups,
    factor,
    entries,
    x_hbm,
    oc_hbm,
    fc_hbm,
    vc_hbm,
    go_hbm,
    bases_hbm,
    fw_hbm,
    vw_hbm,
    ow_hbm,
    m1_hbm,
    m2_hbm,
    all_w,
    dirs,
    b_buf,
    scale_ref,
    n1_ref,
    n2_ref,
    fw_ref,
    vw_ref,
    ow_ref,
    m1_ref,
    m2_ref,
    x_buf,
    oc_buf,
    c_buf,
    acc,
    part,
    got,
    mine,
    sums,
    first_sem,
    load_sem,
    base_sem,
    w_send,
    w_recv,
    part_send,
    part_recv,
    dir_send,
    dir_recv,
    sum_send,
    sum_recv,
):
    me = lax.axis_index("fs")
    mt = lax.axis_index("tp")
    z = lax.div(me, SIDE)
    x = lax.rem(me, SIDE)
    tiles = load_sem.shape[1]
    tokens = x_buf.shape[0]
    rows_t = tokens // tiles
    rank_rows = m1_ref.shape[1]
    own = fw_ref.shape[0]
    half_rows = own // 2

    firsts = [
        pltpu.make_async_copy(src, dst, first_sem.at[i])
        for i, (src, dst) in enumerate(
            (
                (fw_hbm, fw_ref),
                (vw_hbm, vw_ref),
                (ow_hbm, ow_ref),
                (m1_hbm, m1_ref),
                (m2_hbm, m2_ref),
            )
        )
    ]
    for copy in firsts[:3]:
        copy.start()
    base_copies = [
        pltpu.make_async_copy(bases_hbm.at[k], b_buf.at[k], base_sem.at[k]) for k in range(3)
    ]

    def load(which, src, dst, tile):
        at = pl.ds(pl.multiple_of(tile * rows_t, rows_t), rows_t)
        return pltpu.make_async_copy(src.at[at, :], dst.at[at, :], load_sem.at[which, tile])

    streams = (
        (x_hbm, x_buf),
        (fc_hbm, c_buf.at[0]),
        (vc_hbm, c_buf.at[1]),
        (oc_hbm, oc_buf),
        (go_hbm, c_buf.at[2]),
    )
    base_copies[0].start()
    for tile in range(tiles):
        for which in (0, 1):
            load(which, *streams[which], tile).start()
    base_copies[1].start()
    for tile in range(tiles):
        load(2, *streams[2], tile).start()
    base_copies[2].start()
    for tile in range(tiles):
        for which in (3, 4):
            load(which, *streams[which], tile).start()
    for copy in firsts[3:]:
        copy.start()

    barrier = pltpu.get_barrier_semaphore()
    for j in range(1, size):
        pl.semaphore_signal(
            barrier, inc=1, device_id=(lax.rem(me + j, size), mt), device_id_type=MESH
        )
    for j in range(1, groups):
        pl.semaphore_signal(
            barrier, inc=1, device_id=(me, lax.rem(mt + j, groups)), device_id_type=MESH
        )
    for copy in firsts[:3]:
        copy.wait()
    all_w[me, 0] = fw_ref[...].astype(jnp.bfloat16)
    all_w[me, 1] = vw_ref[...].astype(jnp.bfloat16)
    all_w[me, 2, :, :own] = ow_ref[:own, :].astype(jnp.bfloat16)
    all_w[me, 2, :, own:] = ow_ref[own:, :].astype(jnp.bfloat16)

    def node(h, a, b):
        dz, dx = (b, a) if h == 0 else (a, b)
        return lax.rem(z + dz + SIDE, SIDE) * SIDE + lax.rem(x + dx + SIDE, SIDE)

    def w_copy(h, s, slot, owner, quarter, dest):
        start, count = h * half_rows, half_rows
        if quarter is not None:
            count = half_rows // 2
            start = start + quarter * count
        view = all_w.at[owner, :, pl.ds(start, count), :]
        return pltpu.make_async_remote_copy(
            src_ref=view,
            dst_ref=view,
            send_sem=w_send.at[h, s, slot],
            recv_sem=w_recv.at[h, s, slot],
            device_id=(dest, mt),
            device_id_type=MESH,
        )

    def near(h, s):
        return w_copy(h, s, 0, me, None, node(h, STEPS[s], 0))

    def near_on(h, s):
        return w_copy(h, s, 1, node(h, -STEPS[s], 0), s, node(h, STEPS[s], 0))

    def far(h, i, s):
        return w_copy(h, s, 2 + i, node(h, OFFSETS[i], 0), None, node(h, 0, STEPS[s]))

    def far_on(h, i, s):
        return w_copy(h, s, 6 + i, node(h, OFFSETS[i], -STEPS[s]), s, node(h, 0, STEPS[s]))

    def stage_0():
        for h in range(2):
            for s in range(2):
                near(h, s).start()
        for h in range(2):
            for s in range(2):
                far(h, 0, s).start()

    def stage_1():
        for h in range(2):
            for s in range(2):
                near(h, s).wait_recv()
        for h in range(2):
            for s in range(2):
                near_on(h, s).start()
        for i in (1, 2):
            for h in range(2):
                for s in range(2):
                    far(h, i, s).start()

    def stage_2():
        for h in range(2):
            for s in range(2):
                far(h, 0, s).wait_recv()
                far_on(h, 0, s).start()

    def stage_3():
        for h in range(2):
            for s in range(2):
                near_on(h, s).wait_recv()
        for h in range(2):
            for s in range(2):
                far(h, 3, s).start()

    def stage_on(i):
        for h in range(2):
            for s in range(2):
                far(h, i, s).wait_recv()
                far_on(h, i, s).start()

    def stage_last():
        for i in range(4):
            for h in range(2):
                for s in range(2):
                    far_on(h, i, s).wait_recv()

    def part_copy(k, j):
        owner = lax.rem(me + j, size)
        at = pl.ds(pl.multiple_of(owner * rank_rows, rank_rows), rank_rows)
        return pltpu.make_async_remote_copy(
            src_ref=part.at[k, at, :],
            dst_ref=got.at[k, j - 1],
            send_sem=part_send.at[k, j - 1],
            recv_sem=part_recv.at[k, j - 1],
            device_id=(owner, mt),
            device_id_type=MESH,
        )

    own_rows = pl.ds(pl.multiple_of(me * rank_rows, rank_rows), rank_rows)

    def dir_copy(k, j):
        return pltpu.make_async_remote_copy(
            src_ref=mine.at[k],
            dst_ref=dirs.at[k, own_rows, :],
            send_sem=dir_send.at[k, j - 1],
            recv_sem=dir_recv.at[k, j - 1],
            device_id=(lax.rem(me + j, size), mt),
            device_id_type=MESH,
        )

    def combine(k):
        projected = acc[k, own_rows, :] * factor
        for j in range(1, size):
            part_copy(k, j).wait_recv()
            projected = projected + got[k, j - 1].astype(jnp.float32)
        one = 0.9 * m1_ref[k] + 0.1 * projected
        two = 0.9 * m2_ref[k] + 0.1 * projected * projected
        n1_ref[k] = one
        n2_ref[k] = two
        rounded = (one / (jnp.sqrt(two) + 1e-08)).astype(jnp.bfloat16)
        mine[k] = rounded
        dirs[k, own_rows, :] = rounded
        for j in range(1, size):
            dir_copy(k, j).start()

    def compute(k, low, high):
        left_which, right_which = ((0, 1), (0, 2), (3, 4))[k]
        source = x_buf if k < 2 else oc_buf
        if low == 0:
            base_copies[k].wait()
            acc[k] = jnp.zeros(acc.shape[1:], acc.dtype)

        def tile_body(tile, carry):
            at = pl.ds(pl.multiple_of(tile * rows_t, rows_t), rows_t)
            if k != 1:
                load(left_which, *streams[left_which], tile).wait()
            reduced = jnp.dot(
                source[at, :], b_buf[k], preferred_element_type=jnp.float32
            ).astype(jnp.bfloat16)
            load(right_which, *streams[right_which], tile).wait()
            acc[k] += lax.dot_general(
                reduced,
                c_buf[k, at, :],
                (((0,), (0,)), ((), ())),
                preferred_element_type=jnp.float32,
            )
            return carry

        lax.fori_loop(low, high, tile_body, 0)

    def send_parts(k):
        part[k] = (acc[k] * factor).astype(jnp.bfloat16)
        for j in range(1, size):
            part_copy(k, j).start()

    with jax.named_scope("barrier"):
        pl.semaphore_wait(barrier, size - 1 + groups - 1)
    stage_0()
    with jax.named_scope("compute0"):
        compute(0, 0, tiles)
        send_parts(0)
    with jax.named_scope("compute1"):
        compute(1, 0, tiles)
        send_parts(1)
    with jax.named_scope("compute2a"):
        compute(2, 0, tiles // 2)
    with jax.named_scope("combine0"):
        for copy in firsts[3:]:
            copy.wait()
        combine(0)
    with jax.named_scope("compute2b"):
        compute(2, tiles // 2, tiles)
        send_parts(2)
    with jax.named_scope("stage1"):
        stage_1()
    with jax.named_scope("combine1"):
        combine(1)
    with jax.named_scope("combine2"):
        combine(2)
    with jax.named_scope("stage2"):
        stage_2()
    with jax.named_scope("stage3"):
        stage_3()
    with jax.named_scope("stage4"):
        stage_on(1)
        stage_on(2)

    row = lax.broadcasted_iota(jnp.int32, scale_ref.shape, 0)
    tile_sum = jnp.zeros(scale_ref.shape, jnp.float32)
    with jax.named_scope("dirs"):
        for k in range(3):
            for j in range(1, size):
                dir_copy(k, j).wait_recv()
            values = dirs[k].astype(jnp.float32)
            tile_sum = tile_sum + jnp.where(row == k, jnp.sum(values * values), 0.0)
        sums[0] = tile_sum

    def sum_copy(j):
        return pltpu.make_async_remote_copy(
            src_ref=sums.at[0],
            dst_ref=sums.at[j],
            send_sem=sum_send.at[j],
            recv_sem=sum_recv.at[j],
            device_id=(me, lax.rem(mt + j, groups)),
            device_id_type=MESH,
        )

    for j in range(1, groups):
        sum_copy(j).start()
    with jax.named_scope("stage5"):
        stage_on(3)
    with jax.named_scope("sums"):
        total = tile_sum
        for j in range(1, groups):
            sum_copy(j).wait_recv()
            total = total + sums[j]
        scale_ref[...] = lax.rsqrt(total / entries + 1.0)
    with jax.named_scope("stage6"):
        stage_last()

    with jax.named_scope("drain"):
        for h in range(2):
            for s in range(2):
                near(h, s).wait_send()
                near_on(h, s).wait_send()
                for i in range(4):
                    far(h, i, s).wait_send()
                    far_on(h, i, s).wait_send()
        for k in range(3):
            for j in range(1, size):
                part_copy(k, j).wait_send()
                dir_copy(k, j).wait_send()
        for j in range(1, groups):
            sum_copy(j).wait_send()


def exchange(size, groups, x, oc, fc, vc, go, bases, fw, vw, ow, m1, m2):
    tokens, width = x.shape
    rank = bases.shape[2]
    rows, columns = fw.shape
    rank_rows = m1.shape[1]
    tiles = 4
    bf16, f32 = jnp.bfloat16, jnp.float32
    vmem = pl.BlockSpec(memory_space=pltpu.VMEM)
    dma = pltpu.SemaphoreType.DMA
    kernel = functools.partial(
        exchange_kernel,
        size,
        groups,
        float(tokens * size) ** (-0.5),
        float(rank * columns * groups),
    )
    return pl.pallas_call(
        kernel,
        out_shape=(
            pltpu.VMEM((size, 3, rows, columns), bf16),
            pltpu.VMEM((3, rank, columns), bf16),
            pltpu.VMEM(bases.shape, bf16),
            pltpu.VMEM((8, 128), f32),
            pltpu.VMEM(m1.shape, f32),
            pltpu.VMEM(m2.shape, f32),
            pltpu.VMEM(fw.shape, f32),
            pltpu.VMEM(vw.shape, f32),
            pltpu.VMEM(ow.shape, f32),
        ),
        in_specs=[pl.BlockSpec(memory_space=pltpu.HBM)] * 11,
        out_specs=(vmem,) * 9,
        scratch_shapes=[
            pltpu.VMEM(m1.shape, f32),
            pltpu.VMEM(m2.shape, f32),
            pltpu.VMEM(x.shape, bf16),
            pltpu.VMEM(oc.shape, bf16),
            pltpu.VMEM((3, tokens, columns), bf16),
            pltpu.VMEM((3, rank, columns), f32),
            pltpu.VMEM((3, rank, columns), bf16),
            pltpu.VMEM((3, size - 1, rank_rows, columns), bf16),
            pltpu.VMEM((3, rank_rows, columns), bf16),
            pltpu.VMEM((groups, 8, 128), f32),
            dma((5,)),
            dma((5, tiles)),
            dma((3,)),
            dma((2, 2, 10)),
            dma((2, 2, 10)),
            dma((3, size - 1)),
            dma((3, size - 1)),
            dma((3, size - 1)),
            dma((3, size - 1)),
            dma((groups,)),
            dma((groups,)),
        ],
        compiler_params=pltpu.CompilerParams(
            collective_id=0, has_side_effects=True, vmem_limit_bytes=40 * 1024 * 1024
        ),
    )(x, oc, fc, vc, go, bases, fw, vw, ow, m1, m2)


def finish_kernel(
    scale_ref,
    dirs_ref,
    all_w,
    bases_ref,
    fw_ref,
    vw_ref,
    ow_ref,
    n1_ref,
    n2_ref,
    new_f,
    new_v,
    new_o,
    copy_f,
    copy_v,
    copy_o,
    n1_out,
    n2_out,
    step_f,
    step_v,
    step_o,
    cf_buf,
    cv_buf,
    co_buf,
    down_buf,
    across_buf,
    tile_sem,
    own_sem,
):
    tiles = tile_sem.shape[1]
    rows = cf_buf.shape[0] // tiles
    own = fw_ref.shape[0]
    owners = rows // own
    copies = []

    def put(src, dst, sem):
        copy = pltpu.make_async_copy(src, dst, sem)
        copy.start()
        copies.append(copy)

    put(n1_ref, n1_out, own_sem.at[6])
    put(n2_ref, n2_out, own_sem.at[7])

    def down(at, k):
        step = jnp.dot(bases_ref[k, at, :], dirs_ref[k], preferred_element_type=jnp.float32)
        return step * scale_ref[k : k + 1, 0:1]

    def across(at):
        step = lax.dot_general(
            dirs_ref[2],
            bases_ref[2, at, :],
            (((0,), (1,)), ((), ())),
            preferred_element_type=jnp.float32,
        )
        return step * scale_ref[2:3, 0:1]

    for tile in range(tiles):
        at = pl.ds(tile * rows, rows)
        owned = pl.ds(tile * owners, owners)
        for k, buf, out in ((0, cf_buf, copy_f), (1, cv_buf, copy_v)):
            old = all_w[owned, k].reshape(rows, cf_buf.shape[1])
            value = old.astype(jnp.float32) - 0.01 * down(at, k)
            buf[at, :] = value.astype(jnp.bfloat16)
            put(buf.at[at, :], out.at[at, :], tile_sem.at[k, tile])
        step = across(at)
        for i in range(owners):
            lanes = pl.ds(tile * rows + i * own, own)
            for j in range(2):
                old = all_w[tile * owners + i, 2, :, j * own : (j + 1) * own]
                value = old.astype(jnp.float32) - 0.01 * step[
                    j * own : (j + 1) * own, i * own : (i + 1) * own
                ]
                co_buf[pl.ds(j * own, own), lanes] = value.astype(jnp.bfloat16)
        put(co_buf.at[:, at], copy_o.at[:, at], tile_sem.at[2, tile])

    me = pl.ds(pl.multiple_of(lax.axis_index("fs") * own, own), own)
    for k, weight, new, out in ((0, fw_ref, new_f, step_f), (1, vw_ref, new_v, step_v)):
        step = down(me, k)
        down_buf[2 * k] = step
        put(down_buf.at[2 * k], out, own_sem.at[2 * k])
        down_buf[2 * k + 1] = weight[...] - 0.01 * step
        put(down_buf.at[2 * k + 1], new, own_sem.at[2 * k + 1])
    step = across(me)
    across_buf[0] = step
    put(across_buf.at[0], step_o, own_sem.at[4])
    across_buf[1] = ow_ref[...] - 0.01 * step
    put(across_buf.at[1], new_o, own_sem.at[5])

    for copy in copies:
        copy.wait()


def finish(all_w, dirs, bases, scales, one, two, fw, vw, ow):
    tiles = 4
    size, _, rows, columns = all_w.shape
    depth = size * rows
    rank = bases.shape[2]
    bf16, f32 = jnp.bfloat16, jnp.float32
    dma = pltpu.SemaphoreType.DMA
    tall = jax.ShapeDtypeStruct((depth, columns), bf16)
    wide = jax.ShapeDtypeStruct((columns, depth), bf16)
    down = jax.ShapeDtypeStruct((rows, columns), f32)
    across = jax.ShapeDtypeStruct((columns, rows), f32)
    small = jax.ShapeDtypeStruct(one.shape, f32)
    return pl.pallas_call(
        finish_kernel,
        out_shape=(down, down, across, tall, tall, wide, small, small, down, down, across),
        in_specs=[pl.BlockSpec(memory_space=pltpu.VMEM)] * 9,
        out_specs=(pl.BlockSpec(memory_space=pltpu.HBM),) * 11,
        scratch_shapes=[
            pltpu.VMEM(tall.shape, bf16),
            pltpu.VMEM(tall.shape, bf16),
            pltpu.VMEM(wide.shape, bf16),
            pltpu.VMEM((4,) + down.shape, f32),
            pltpu.VMEM((2,) + across.shape, f32),
            dma((3, tiles)),
            dma((8,)),
        ],
        compiler_params=pltpu.CompilerParams(vmem_limit_bytes=24 * 1024 * 1024),
        cost_estimate=pl.CostEstimate(
            flops=6 * depth * rank * columns, bytes_accessed=8 * depth * columns, transcendentals=0
        ),
    )(scales, dirs, all_w, bases, fw, vw, ow, one, two)


def on_device(
    normed_input,
    forget_cot,
    value_cot,
    gated_output,
    output_cot,
    forget_weight,
    value_weight,
    out_weight,
    bases,
    first_moment,
    second_moment,
):
    size, groups = lax.axis_size("fs"), lax.axis_size("tp")
    held = exchange(
        size,
        groups,
        normed_input,
        output_cot,
        forget_cot,
        value_cot,
        gated_output,
        bases,
        forget_weight,
        value_weight,
        out_weight,
        first_moment.transpose(1, 0, 2),
        second_moment.transpose(1, 0, 2),
    )
    outs = finish(*held)
    return (
        *outs[:6],
        outs[6].transpose(1, 0, 2),
        outs[7].transpose(1, 0, 2),
        *outs[8:],
    )


def solution(mesh):
    placed = (
        P("fs", None),
        P("fs", "tp"),
        P("fs", "tp"),
        P("fs", "tp"),
        P("fs", None),
        P("fs", "tp"),
        P("fs", "tp"),
        P("tp", "fs"),
        P(),
        P("fs", None, "tp"),
        P("fs", None, "tp"),
    )
    return jax.shard_map(
        on_device,
        mesh=mesh,
        in_specs=placed,
        out_specs=(
            P("fs", "tp"),
            P("fs", "tp"),
            P("tp", "fs"),
            P(None, "tp"),
            P(None, "tp"),
            P("tp", None),
            P("fs", None, "tp"),
            P("fs", None, "tp"),
            P("fs", "tp"),
            P("fs", "tp"),
            P("tp", "fs"),
        ),
        check_vma=False,
    )
```

```python
import functools

import jax
import jax.numpy as jnp
from jax import lax
from jax.experimental import pallas as pl
from jax.experimental.pallas import tpu as pltpu
from jax.sharding import PartitionSpec as P

MESH = pl.DeviceIdType.MESH
SIDE = 4
STEPS = (1, -1)
OFFSETS = (0, -1, 1, 2)


def exchange_kernel(
    size,
    groups,
    factor,
    entries,
    x_hbm,
    oc_hbm,
    fc_hbm,
    vc_hbm,
    go_hbm,
    bases_hbm,
    fw_hbm,
    vw_hbm,
    ow_hbm,
    m1_hbm,
    m2_hbm,
    all_w,
    dirs,
    b_buf,
    scale_ref,
    n1_ref,
    n2_ref,
    fw_ref,
    vw_ref,
    ow_ref,
    m1_ref,
    m2_ref,
    x_buf,
    oc_buf,
    c_buf,
    red,
    acc,
    part,
    got,
    mine,
    sums,
    first_sem,
    load_sem,
    cot_sem,
    base_sem,
    pair_send,
    pair_recv,
    w_send,
    w_recv,
    part_send,
    part_recv,
    dir_send,
    dir_recv,
    sum_send,
    sum_recv,
):
    me = lax.axis_index("fs")
    mt = lax.axis_index("tp")
    z = lax.div(me, SIDE)
    x = lax.rem(me, SIDE)
    core = lax.rem(mt, 2)
    partner = mt + 1 - 2 * core
    tiles = load_sem.shape[1]
    tokens = c_buf.shape[1]
    rows_t = x_buf.shape[0] // tiles
    first_row = core * x_buf.shape[0]
    rank_rows = m1_ref.shape[1]
    own = fw_ref.shape[0]
    half_rows = own // 2

    firsts = [
        pltpu.make_async_copy(src, dst, first_sem.at[i])
        for i, (src, dst) in enumerate(
            (
                (fw_hbm, fw_ref),
                (vw_hbm, vw_ref),
                (ow_hbm, ow_ref),
                (m1_hbm, m1_ref),
                (m2_hbm, m2_ref),
            )
        )
    ]
    for copy in firsts[:3]:
        copy.start()
    base_copies = [
        pltpu.make_async_copy(bases_hbm.at[k], b_buf.at[k], base_sem.at[k]) for k in range(3)
    ]

    def tile_rows(tile):
        return pl.ds(pl.multiple_of(first_row + tile * rows_t, rows_t), rows_t)

    def load(which, src, dst, tile):
        held = pl.ds(tile * rows_t, rows_t)
        return pltpu.make_async_copy(
            src.at[tile_rows(tile), :], dst.at[held, :], load_sem.at[which, tile]
        )

    def load_all(k):
        return pltpu.make_async_copy((fc_hbm, vc_hbm, go_hbm)[k], c_buf.at[k], cot_sem.at[k])

    streams = ((x_hbm, x_buf), (oc_hbm, oc_buf))
    base_copies[0].start()
    base_copies[1].start()
    load(0, *streams[0], 0).start()

    barrier = pltpu.get_barrier_semaphore()
    for j in range(1, size):
        pl.semaphore_signal(
            barrier, inc=1, device_id=(lax.rem(me + j, size), mt), device_id_type=MESH
        )
    for j in range(1, groups):
        pl.semaphore_signal(
            barrier, inc=1, device_id=(me, lax.rem(mt + j, groups)), device_id_type=MESH
        )
    for copy in firsts[:3]:
        copy.wait()
    for tile in range(1, tiles):
        load(0, *streams[0], tile).start()
    base_copies[2].start()
    for tile in range(tiles):
        load(1, *streams[1], tile).start()
    for k in range(3):
        load_all(k).start()
    for copy in firsts[3:]:
        copy.start()
    all_w[me, 0] = fw_ref[...].astype(jnp.bfloat16)
    all_w[me, 1] = vw_ref[...].astype(jnp.bfloat16)
    all_w[me, 2, :, :own] = ow_ref[:own, :].astype(jnp.bfloat16)
    all_w[me, 2, :, own:] = ow_ref[own:, :].astype(jnp.bfloat16)

    def node(h, a, b):
        dz, dx = (b, a) if h == 0 else (a, b)
        return lax.rem(z + dz + SIDE, SIDE) * SIDE + lax.rem(x + dx + SIDE, SIDE)

    def w_copy(h, s, slot, owner, quarter, dest):
        start, count = h * half_rows, half_rows
        if quarter is not None:
            count = half_rows // 2
            start = start + quarter * count
        view = all_w.at[owner, :, pl.ds(start, count), :]
        return pltpu.make_async_remote_copy(
            src_ref=view,
            dst_ref=view,
            send_sem=w_send.at[h, s, slot],
            recv_sem=w_recv.at[h, s, slot],
            device_id=(dest, mt),
            device_id_type=MESH,
        )

    def near(h, s):
        return w_copy(h, s, 0, me, None, node(h, STEPS[s], 0))

    def near_on(h, s):
        return w_copy(h, s, 1, node(h, -STEPS[s], 0), s, node(h, STEPS[s], 0))

    def far(h, i, s):
        return w_copy(h, s, 2 + i, node(h, OFFSETS[i], 0), None, node(h, 0, STEPS[s]))

    def far_on(h, i, s):
        return w_copy(h, s, 6 + i, node(h, OFFSETS[i], -STEPS[s]), s, node(h, 0, STEPS[s]))

    def stage_0():
        for h in range(2):
            for s in range(2):
                near(h, s).start()
        for h in range(2):
            for s in range(2):
                far(h, 0, s).start()

    def stage_1():
        for h in range(2):
            for s in range(2):
                near(h, s).wait_recv()
        for h in range(2):
            for s in range(2):
                near_on(h, s).start()

    def stage_far(i):
        for h in range(2):
            for s in range(2):
                far(h, i, s).start()

    def stage_2():
        for h in range(2):
            for s in range(2):
                far(h, 0, s).wait_recv()
                far_on(h, 0, s).start()

    def stage_3():
        for h in range(2):
            for s in range(2):
                near_on(h, s).wait_recv()
        stage_far(3)

    def stage_on(i):
        for h in range(2):
            for s in range(2):
                far(h, i, s).wait_recv()
                far_on(h, i, s).start()

    def stage_last():
        for i in range(4):
            for h in range(2):
                for s in range(2):
                    far_on(h, i, s).wait_recv()

    def part_copy(k, j):
        owner = lax.rem(me + j, size)
        at = pl.ds(pl.multiple_of(owner * rank_rows, rank_rows), rank_rows)
        return pltpu.make_async_remote_copy(
            src_ref=part.at[k, at, :],
            dst_ref=got.at[k, j - 1],
            send_sem=part_send.at[k, j - 1],
            recv_sem=part_recv.at[k, j - 1],
            device_id=(owner, mt),
            device_id_type=MESH,
        )

    own_rows = pl.ds(pl.multiple_of(me * rank_rows, rank_rows), rank_rows)

    def dir_copy(k, j):
        return pltpu.make_async_remote_copy(
            src_ref=mine.at[k],
            dst_ref=dirs.at[k, own_rows, :],
            send_sem=dir_send.at[k, j - 1],
            recv_sem=dir_recv.at[k, j - 1],
            device_id=(lax.rem(me + j, size), mt),
            device_id_type=MESH,
        )

    def combine(k):
        projected = acc[k, own_rows, :] * factor
        for j in range(1, size):
            part_copy(k, j).wait_recv()
            projected = projected + got[k, j - 1].astype(jnp.float32)
        one = 0.9 * m1_ref[k] + 0.1 * projected
        two = 0.9 * m2_ref[k] + 0.1 * projected * projected
        n1_ref[k] = one
        n2_ref[k] = two
        rounded = (one / (jnp.sqrt(two) + 1e-08)).astype(jnp.bfloat16)
        mine[k] = rounded
        dirs[k, own_rows, :] = rounded
        for j in range(1, size):
            dir_copy(k, j).start()

    def pair_copy(k, tile):
        view = red.at[k, tile_rows(tile), :]
        return pltpu.make_async_remote_copy(
            src_ref=view,
            dst_ref=view,
            send_sem=pair_send.at[k, tile],
            recv_sem=pair_recv.at[k, tile],
            device_id=(me, partner),
            device_id_type=MESH,
        )

    def reduce_pair(tile):
        load(0, *streams[0], tile).wait()
        rows = x_buf[pl.ds(tile * rows_t, rows_t), :]
        first = jnp.dot(rows, b_buf[0], preferred_element_type=jnp.float32)
        second = jnp.dot(rows, b_buf[1], preferred_element_type=jnp.float32)
        red[0, tile_rows(tile), :] = first.astype(jnp.bfloat16)
        red[1, tile_rows(tile), :] = second.astype(jnp.bfloat16)
        for k in range(2):
            pair_copy(k, tile).start()

    def reduce_last(tile):
        load(1, *streams[1], tile).wait()
        half = rows_t // 2
        upper, lower = pl.ds(tile * rows_t, half), pl.ds(tile * rows_t + half, half)
        first = jnp.dot(oc_buf[upper, :], b_buf[2], preferred_element_type=jnp.float32)
        second = jnp.dot(oc_buf[lower, :], b_buf[2], preferred_element_type=jnp.float32)
        both = jnp.concatenate([first, second], axis=0)
        red[2, tile_rows(tile), :] = both.astype(jnp.bfloat16)
        pair_copy(2, tile).start()

    def fold(left, right):
        return lax.dot_general(
            left, right, (((0,), (0,)), ((), ())), preferred_element_type=jnp.float32
        )

    def project_pair():
        for k in range(2):
            load_all(k).wait()
            for tile in range(tiles):
                pair_copy(k, tile).wait_recv()
        first = fold(red[0], c_buf[0])
        second = fold(red[1], c_buf[1])
        acc[0] = first
        acc[1] = second
        part[0] = (first * factor).astype(jnp.bfloat16)
        part[1] = (second * factor).astype(jnp.bfloat16)

    def project_last():
        load_all(2).wait()
        for tile in range(tiles):
            pair_copy(2, tile).wait_recv()
        half = tokens // 2
        total = fold(red[2, :half, :], c_buf[2, :half, :])
        total = total + fold(red[2, half:, :], c_buf[2, half:, :])
        acc[2] = total
        part[2] = (total * factor).astype(jnp.bfloat16)

    def send_parts(k):
        for j in range(1, size):
            part_copy(k, j).start()

    with jax.named_scope("barrier"):
        pl.semaphore_wait(barrier, size - 1 + groups - 1)
    stage_0()
    with jax.named_scope("compute0"):
        for k in range(2):
            base_copies[k].wait()
        for tile in range(tiles):
            reduce_pair(tile)
    with jax.named_scope("compute2"):
        base_copies[2].wait()
        for tile in range(tiles):
            reduce_last(tile)
    stage_1()
    with jax.named_scope("project0"):
        project_pair()
        send_parts(0)
        send_parts(1)
    with jax.named_scope("project2"):
        project_last()
        send_parts(2)
    stage_far(1)
    for copy in firsts[3:]:
        copy.wait()
    with jax.named_scope("combine0"):
        combine(0)
    with jax.named_scope("combine1"):
        combine(1)
    with jax.named_scope("combine2"):
        combine(2)
    with jax.named_scope("stage2"):
        stage_far(2)
        stage_2()
    with jax.named_scope("stage3"):
        stage_3()
    with jax.named_scope("stage4"):
        stage_on(1)

    row = lax.broadcasted_iota(jnp.int32, scale_ref.shape, 0)
    tile_sum = jnp.zeros(scale_ref.shape, jnp.float32)
    with jax.named_scope("dirs"):
        for k in range(3):
            for j in range(1, size):
                dir_copy(k, j).wait_recv()
            values = dirs[k].astype(jnp.float32)
            tile_sum = tile_sum + jnp.where(row == k, jnp.sum(values * values), 0.0)
        sums[0] = tile_sum

    def sum_copy(j):
        return pltpu.make_async_remote_copy(
            src_ref=sums.at[0],
            dst_ref=sums.at[j],
            send_sem=sum_send.at[j],
            recv_sem=sum_recv.at[j],
            device_id=(me, lax.rem(mt + j, groups)),
            device_id_type=MESH,
        )

    for j in range(1, groups):
        sum_copy(j).start()
    with jax.named_scope("stage5"):
        stage_on(2)
        stage_on(3)
    with jax.named_scope("sums"):
        total = tile_sum
        for j in range(1, groups):
            sum_copy(j).wait_recv()
            total = total + sums[j]
        scale_ref[...] = lax.rsqrt(total / entries + 1.0)
    with jax.named_scope("stage6"):
        stage_last()

    with jax.named_scope("drain"):
        for h in range(2):
            for s in range(2):
                near(h, s).wait_send()
                near_on(h, s).wait_send()
                for i in range(4):
                    far(h, i, s).wait_send()
                    far_on(h, i, s).wait_send()
        for k in range(3):
            for j in range(1, size):
                part_copy(k, j).wait_send()
                dir_copy(k, j).wait_send()
            for tile in range(tiles):
                pair_copy(k, tile).wait_send()
        for j in range(1, groups):
            sum_copy(j).wait_send()


def exchange(size, groups, x, oc, fc, vc, go, bases, fw, vw, ow, m1, m2):
    tokens, width = x.shape
    rank = bases.shape[2]
    rows, columns = fw.shape
    rank_rows = m1.shape[1]
    tiles = 2
    bf16, f32 = jnp.bfloat16, jnp.float32
    vmem = pl.BlockSpec(memory_space=pltpu.VMEM)
    dma = pltpu.SemaphoreType.DMA
    kernel = functools.partial(
        exchange_kernel,
        size,
        groups,
        float(tokens * size) ** (-0.5),
        float(rank * columns * groups),
    )
    return pl.pallas_call(
        kernel,
        out_shape=(
            pltpu.VMEM((size, 3, rows, columns), bf16),
            pltpu.VMEM((3, rank, columns), bf16),
            pltpu.VMEM(bases.shape, bf16),
            pltpu.VMEM((8, 128), f32),
            pltpu.VMEM(m1.shape, f32),
            pltpu.VMEM(m2.shape, f32),
            pltpu.VMEM(fw.shape, f32),
            pltpu.VMEM(vw.shape, f32),
            pltpu.VMEM(ow.shape, f32),
        ),
        in_specs=[pl.BlockSpec(memory_space=pltpu.HBM)] * 11,
        out_specs=(vmem,) * 9,
        scratch_shapes=[
            pltpu.VMEM(m1.shape, f32),
            pltpu.VMEM(m2.shape, f32),
            pltpu.VMEM((tokens // 2, width), bf16),
            pltpu.VMEM((tokens // 2, width), bf16),
            pltpu.VMEM((3, tokens, columns), bf16),
            pltpu.VMEM((3, tokens, rank), bf16),
            pltpu.VMEM((3, rank, columns), f32),
            pltpu.VMEM((3, rank, columns), bf16),
            pltpu.VMEM((3, size - 1, rank_rows, columns), bf16),
            pltpu.VMEM((3, rank_rows, columns), bf16),
            pltpu.VMEM((groups, 8, 128), f32),
            dma((5,)),
            dma((2, tiles)),
            dma((3,)),
            dma((3,)),
            dma((3, tiles)),
            dma((3, tiles)),
            dma((2, 2, 10)),
            dma((2, 2, 10)),
            dma((3, size - 1)),
            dma((3, size - 1)),
            dma((3, size - 1)),
            dma((3, size - 1)),
            dma((groups,)),
            dma((groups,)),
        ],
        compiler_params=pltpu.CompilerParams(
            collective_id=0, has_side_effects=True, vmem_limit_bytes=52 * 1024 * 1024
        ),
    )(x, oc, fc, vc, go, bases, fw, vw, ow, m1, m2)


def finish_kernel(
    scale_ref,
    dirs_ref,
    all_w,
    bases_ref,
    fw_ref,
    vw_ref,
    ow_ref,
    n1_ref,
    n2_ref,
    new_f,
    new_v,
    new_o,
    copy_f,
    copy_v,
    copy_o,
    n1_out,
    n2_out,
    step_f,
    step_v,
    step_o,
    cf_buf,
    cv_buf,
    co_buf,
    down_buf,
    across_buf,
    tile_sem,
    own_sem,
):
    tiles = tile_sem.shape[1]
    rows = cf_buf.shape[0] // tiles
    own = fw_ref.shape[0]
    owners = rows // own
    copies = []

    def put(src, dst, sem):
        copy = pltpu.make_async_copy(src, dst, sem)
        copy.start()
        copies.append(copy)

    put(n1_ref, n1_out, own_sem.at[6])
    put(n2_ref, n2_out, own_sem.at[7])

    def down(at, k):
        step = jnp.dot(bases_ref[k, at, :], dirs_ref[k], preferred_element_type=jnp.float32)
        return step * scale_ref[k : k + 1, 0:1]

    def across(at):
        step = lax.dot_general(
            dirs_ref[2],
            bases_ref[2, at, :],
            (((0,), (1,)), ((), ())),
            preferred_element_type=jnp.float32,
        )
        return step * scale_ref[2:3, 0:1]

    for tile in range(tiles):
        at = pl.ds(tile * rows, rows)
        owned = pl.ds(tile * owners, owners)
        for k, buf, out in ((0, cf_buf, copy_f), (1, cv_buf, copy_v)):
            old = all_w[owned, k].reshape(rows, cf_buf.shape[1])
            value = old.astype(jnp.float32) - 0.01 * down(at, k)
            buf[at, :] = value.astype(jnp.bfloat16)
            put(buf.at[at, :], out.at[at, :], tile_sem.at[k, tile])
        step = across(at)
        for i in range(owners):
            lanes = pl.ds(tile * rows + i * own, own)
            for j in range(2):
                old = all_w[tile * owners + i, 2, :, j * own : (j + 1) * own]
                value = old.astype(jnp.float32) - 0.01 * step[
                    j * own : (j + 1) * own, i * own : (i + 1) * own
                ]
                co_buf[pl.ds(j * own, own), lanes] = value.astype(jnp.bfloat16)
        put(co_buf.at[:, at], copy_o.at[:, at], tile_sem.at[2, tile])

    me = pl.ds(pl.multiple_of(lax.axis_index("fs") * own, own), own)
    for k, weight, new, out in ((0, fw_ref, new_f, step_f), (1, vw_ref, new_v, step_v)):
        step = down(me, k)
        down_buf[2 * k] = step
        put(down_buf.at[2 * k], out, own_sem.at[2 * k])
        down_buf[2 * k + 1] = weight[...] - 0.01 * step
        put(down_buf.at[2 * k + 1], new, own_sem.at[2 * k + 1])
    step = across(me)
    across_buf[0] = step
    put(across_buf.at[0], step_o, own_sem.at[4])
    across_buf[1] = ow_ref[...] - 0.01 * step
    put(across_buf.at[1], new_o, own_sem.at[5])

    for copy in copies:
        copy.wait()


def finish(all_w, dirs, bases, scales, one, two, fw, vw, ow):
    tiles = 4
    size, _, rows, columns = all_w.shape
    depth = size * rows
    rank = bases.shape[2]
    bf16, f32 = jnp.bfloat16, jnp.float32
    dma = pltpu.SemaphoreType.DMA
    tall = jax.ShapeDtypeStruct((depth, columns), bf16)
    wide = jax.ShapeDtypeStruct((columns, depth), bf16)
    down = jax.ShapeDtypeStruct((rows, columns), f32)
    across = jax.ShapeDtypeStruct((columns, rows), f32)
    small = jax.ShapeDtypeStruct(one.shape, f32)
    return pl.pallas_call(
        finish_kernel,
        out_shape=(down, down, across, tall, tall, wide, small, small, down, down, across),
        in_specs=[pl.BlockSpec(memory_space=pltpu.VMEM)] * 9,
        out_specs=(pl.BlockSpec(memory_space=pltpu.HBM),) * 11,
        scratch_shapes=[
            pltpu.VMEM(tall.shape, bf16),
            pltpu.VMEM(tall.shape, bf16),
            pltpu.VMEM(wide.shape, bf16),
            pltpu.VMEM((4,) + down.shape, f32),
            pltpu.VMEM((2,) + across.shape, f32),
            dma((3, tiles)),
            dma((8,)),
        ],
        compiler_params=pltpu.CompilerParams(vmem_limit_bytes=24 * 1024 * 1024),
        cost_estimate=pl.CostEstimate(
            flops=6 * depth * rank * columns, bytes_accessed=8 * depth * columns, transcendentals=0
        ),
    )(scales, dirs, all_w, bases, fw, vw, ow, one, two)


def on_device(
    normed_input,
    forget_cot,
    value_cot,
    gated_output,
    output_cot,
    forget_weight,
    value_weight,
    out_weight,
    bases,
    first_moment,
    second_moment,
):
    size, groups = lax.axis_size("fs"), lax.axis_size("tp")
    held = exchange(
        size,
        groups,
        normed_input,
        output_cot,
        forget_cot,
        value_cot,
        gated_output,
        bases,
        forget_weight,
        value_weight,
        out_weight,
        first_moment.transpose(1, 0, 2),
        second_moment.transpose(1, 0, 2),
    )
    outs = finish(*held)
    return (
        *outs[:6],
        outs[6].transpose(1, 0, 2),
        outs[7].transpose(1, 0, 2),
        *outs[8:],
    )


def solution(mesh):
    placed = (
        P("fs", None),
        P("fs", "tp"),
        P("fs", "tp"),
        P("fs", "tp"),
        P("fs", None),
        P("fs", "tp"),
        P("fs", "tp"),
        P("tp", "fs"),
        P(),
        P("fs", None, "tp"),
        P("fs", None, "tp"),
    )
    return jax.shard_map(
        on_device,
        mesh=mesh,
        in_specs=placed,
        out_specs=(
            P("fs", "tp"),
            P("fs", "tp"),
            P("tp", "fs"),
            P(None, "tp"),
            P(None, "tp"),
            P("tp", None),
            P("fs", None, "tp"),
            P("fs", None, "tp"),
            P("fs", "tp"),
            P("fs", "tp"),
            P("tp", "fs"),
        ),
        check_vma=False,
    )
```

```python
import functools

import jax
import jax.numpy as jnp
from jax import lax
from jax.experimental import pallas as pl
from jax.experimental.pallas import tpu as pltpu
from jax.sharding import PartitionSpec as P

MESH = pl.DeviceIdType.MESH
SIDE = 4
STEPS = (1, -1)
OFFSETS = (0, -1, 1, 2)


def exchange_kernel(
    size,
    groups,
    factor,
    entries,
    x_hbm,
    oc_hbm,
    fc_hbm,
    vc_hbm,
    go_hbm,
    bases_hbm,
    fw_hbm,
    vw_hbm,
    ow_hbm,
    m1_hbm,
    m2_hbm,
    all_w,
    dirs,
    b_buf,
    scale_ref,
    n1_ref,
    n2_ref,
    fw_ref,
    vw_ref,
    ow_ref,
    m1_ref,
    m2_ref,
    x_buf,
    oc_buf,
    c_buf,
    red,
    acc,
    part,
    got,
    held,
    mid,
    last,
    sums,
    totals,
    first_sem,
    load_sem,
    cot_sem,
    base_sem,
    pair_recv,
    send_sem,
    w_recv,
    part_recv,
    dir_recv,
    sum_recv,
):
    me = lax.axis_index("fs")
    mt = lax.axis_index("tp")
    z = lax.div(me, SIDE)
    x = lax.rem(me, SIDE)
    core = lax.rem(mt, 2)
    partner = mt + 1 - 2 * core
    tiles = load_sem.shape[1]
    tokens = c_buf.shape[1]
    rows_t = x_buf.shape[0] // tiles
    first_row = core * x_buf.shape[0]
    rank_rows = m1_ref.shape[1]
    columns = m1_ref.shape[2]
    own = fw_ref.shape[0]
    half_rows = own // 2

    firsts = [
        pltpu.make_async_copy(src, dst, first_sem.at[i])
        for i, (src, dst) in enumerate(
            (
                (fw_hbm, fw_ref),
                (vw_hbm, vw_ref),
                (ow_hbm, ow_ref),
                (m1_hbm, m1_ref),
                (m2_hbm, m2_ref),
            )
        )
    ]
    for copy in firsts[:3]:
        copy.start()
    base_copies = [
        pltpu.make_async_copy(bases_hbm.at[k], b_buf.at[k], base_sem.at[k]) for k in range(3)
    ]

    def tile_rows(tile):
        return pl.ds(pl.multiple_of(first_row + tile * rows_t, rows_t), rows_t)

    def load(which, src, dst, tile):
        held = pl.ds(tile * rows_t, rows_t)
        return pltpu.make_async_copy(
            src.at[tile_rows(tile), :], dst.at[held, :], load_sem.at[which, tile]
        )

    def load_all(k):
        return pltpu.make_async_copy((fc_hbm, vc_hbm, go_hbm)[k], c_buf.at[k], cot_sem.at[k])

    streams = ((x_hbm, x_buf), (oc_hbm, oc_buf))
    base_copies[0].start()
    base_copies[1].start()
    load(0, *streams[0], 0).start()

    barrier = pltpu.get_barrier_semaphore()
    for j in range(1, size):
        pl.semaphore_signal(
            barrier, inc=1, device_id=(lax.rem(me + j, size), mt), device_id_type=MESH
        )
    for j in range(1, groups):
        pl.semaphore_signal(
            barrier, inc=1, device_id=(me, lax.rem(mt + j, groups)), device_id_type=MESH
        )
    for copy in firsts[:3]:
        copy.wait()
    for tile in range(1, tiles):
        load(0, *streams[0], tile).start()
    base_copies[2].start()
    for tile in range(tiles):
        load(1, *streams[1], tile).start()
    for k in range(3):
        load_all(k).start()
    for copy in firsts[3:]:
        copy.start()
    all_w[me, 0] = fw_ref[...].astype(jnp.bfloat16)
    all_w[me, 1] = vw_ref[...].astype(jnp.bfloat16)
    all_w[me, 2, :, :own] = ow_ref[:own, :].astype(jnp.bfloat16)
    all_w[me, 2, :, own:] = ow_ref[own:, :].astype(jnp.bfloat16)

    def node(h, a, b):
        dz, dx = (b, a) if h == 0 else (a, b)
        return lax.rem(z + dz + SIDE, SIDE) * SIDE + lax.rem(x + dx + SIDE, SIDE)

    def w_copy(h, slot, owner, quarter, dest):
        start, count = h * half_rows, half_rows
        if quarter is not None:
            count = half_rows // 2
            start = start + quarter * count
        view = all_w.at[owner, :, pl.ds(start, count), :]
        return pltpu.make_async_remote_copy(
            src_ref=view,
            dst_ref=view,
            send_sem=send_sem.at[0],
            recv_sem=w_recv.at[slot],
            device_id=(dest, mt),
            device_id_type=MESH,
        )

    def near(h, s):
        return w_copy(h, 0, me, None, node(h, STEPS[s], 0))

    def near_on(h, s):
        return w_copy(h, 1, node(h, -STEPS[s], 0), s, node(h, STEPS[s], 0))

    def far(h, i, s):
        return w_copy(h, 2 + i, node(h, OFFSETS[i], 0), None, node(h, 0, STEPS[s]))

    def far_on(h, i, s):
        return w_copy(h, 6, node(h, OFFSETS[i], -STEPS[s]), s, node(h, 0, STEPS[s]))

    def all_of(view, send, recv, to=None):
        return pltpu.make_async_remote_copy(
            src_ref=view,
            dst_ref=view,
            send_sem=send_sem.at[send],
            recv_sem=recv,
            device_id=(node(0, 1, 0), mt) if to is None else to,
            device_id_type=MESH,
        )

    def w_arrived(slot):
        count = (2, 1, 2, 2, 2, 2, 4)[slot]
        all_of(all_w.at[pl.ds(0, count)], 0, w_recv.at[slot]).wait_recv()

    def each(start):
        for h in range(2):
            for s in range(2):
                start(h, s).start()

    def stage_0():
        each(near)
        stage_far(0)

    def stage_1():
        w_arrived(0)
        each(near_on)

    def stage_far(i):
        each(lambda h, s: far(h, i, s))

    def stage_on(i):
        w_arrived(2 + i)
        each(lambda h, s: far_on(h, i, s))

    def stage_3():
        w_arrived(1)
        stage_far(3)

    half_cols = columns // 2

    def cut(h):
        return pl.ds(h * half_cols, half_cols)

    def line(h, second, j):
        first_axis = (h == 0) != second
        return (
            z * SIDE + lax.rem(x + j, SIDE) if first_axis else lax.rem(z + j, SIDE) * SIDE + x
        )

    def blocks(ref, k, h, j):
        if h == 0:
            return ref.at[k, :, lax.rem(x + j, SIDE), :, cut(h)]
        return ref.at[k, lax.rem(z + j, SIDE), :, :, cut(h)]

    def move(src, dst, send, recv, dest):
        return pltpu.make_async_remote_copy(
            src_ref=src,
            dst_ref=dst,
            send_sem=send_sem.at[send],
            recv_sem=recv,
            device_id=(dest, mt),
            device_id_type=MESH,
        )

    def part_first(k, h, j):
        return move(
            blocks(part, k, h, j), got.at[k, h, j - 1], 1, part_recv.at[0, k // 2], line(h, False, j)
        )

    def part_second(k, h, j):
        place = lax.rem((z if h == 0 else x) + j, SIDE)
        return move(
            mid.at[k, h, place], last.at[k, h, j - 1], 2, part_recv.at[1, k // 2], line(h, True, j)
        )

    def dir_first(k, h, j):
        view = dirs.at[k, z, x, :, cut(h)]
        return move(view, view, 3, dir_recv.at[0], line(h, False, j))

    def dir_second(k, h, j):
        view = dirs.at[k, z, :, :, cut(h)] if h == 0 else dirs.at[k, :, x, :, cut(h)]
        return move(view, view, 4, dir_recv.at[1], line(h, True, j))

    def group_of(ref, ks):
        return ref.at[pl.ds(ks[0], len(ks))]

    ALL = [(h, j) for h in range(2) for j in range(1, SIDE)]

    def send_parts(k):
        for h, j in ALL:
            part_first(k, h, j).start()

    def pass_parts(ks):
        all_of(group_of(got, ks), 1, part_recv.at[0, ks[0] // 2]).wait_recv()
        for k in ks:
            for h in range(2):
                own_part = acc[k, :, x, :, cut(h)] if h == 0 else acc[k, z, :, :, cut(h)]
                total = own_part * factor
                for j in range(1, SIDE):
                    total = total + got[k, h, j - 1].astype(jnp.float32)
                held[k, h] = total
                mid[k, h] = total.astype(jnp.bfloat16)
                for j in range(1, SIDE):
                    part_second(k, h, j).start()

    lane = lax.broadcasted_iota(jnp.int32, sums.shape[1:], 1)

    def combine(ks):
        all_of(group_of(last, ks), 2, part_recv.at[1, ks[0] // 2]).wait_recv()
        return sum(update(k) for k in ks)

    def update(k):
        square = jnp.zeros((rank_rows, half_cols), jnp.float32)
        for h in range(2):
            projected = held[k, h, z if h == 0 else x]
            for j in range(1, SIDE):
                projected = projected + last[k, h, j - 1].astype(jnp.float32)
            one = 0.9 * m1_ref[k, :, cut(h)] + 0.1 * projected
            two = 0.9 * m2_ref[k, :, cut(h)] + 0.1 * projected * projected
            n1_ref[k, :, cut(h)] = one
            n2_ref[k, :, cut(h)] = two
            rounded = (one / (jnp.sqrt(two) + 1e-08)).astype(jnp.bfloat16)
            dirs[k, z, x, :, cut(h)] = rounded
            for j in range(1, SIDE):
                dir_first(k, h, j).start()
            value = rounded.astype(jnp.float32)
            square = square + value * value
        return jnp.where(lane == k, jnp.sum(square), 0.0)

    def pass_dirs():
        all_of(last, 3, dir_recv.at[0]).wait_recv()
        for k in range(3):
            for h, j in ALL:
                dir_second(k, h, j).start()

    def pair_copy(k, tile):
        view = red.at[k, tile_rows(tile), :]
        return pltpu.make_async_remote_copy(
            src_ref=view,
            dst_ref=view,
            send_sem=send_sem.at[5],
            recv_sem=pair_recv.at[k // 2],
            device_id=(me, partner),
            device_id_type=MESH,
        )

    def pair_half(ks, recv):
        view = red.at[ks, pl.ds(0, tokens // 2), :]
        return all_of(view, 5, recv, (me, partner))

    def reduce_pair(tile):
        load(0, *streams[0], tile).wait()
        rows = x_buf[pl.ds(tile * rows_t, rows_t), :]
        first = jnp.dot(rows, b_buf[0], preferred_element_type=jnp.float32)
        second = jnp.dot(rows, b_buf[1], preferred_element_type=jnp.float32)
        red[0, tile_rows(tile), :] = first.astype(jnp.bfloat16)
        red[1, tile_rows(tile), :] = second.astype(jnp.bfloat16)
        for k in range(2):
            pair_copy(k, tile).start()

    def reduce_last(tile):
        load(1, *streams[1], tile).wait()
        half = rows_t // 2
        upper, lower = pl.ds(tile * rows_t, half), pl.ds(tile * rows_t + half, half)
        first = jnp.dot(oc_buf[upper, :], b_buf[2], preferred_element_type=jnp.float32)
        second = jnp.dot(oc_buf[lower, :], b_buf[2], preferred_element_type=jnp.float32)
        both = jnp.concatenate([first, second], axis=0)
        red[2, tile_rows(tile), :] = both.astype(jnp.bfloat16)
        pair_copy(2, tile).start()

    def fold(left, right):
        return lax.dot_general(
            left, right, (((0,), (0,)), ((), ())), preferred_element_type=jnp.float32
        )

    def project_pair():
        for k in range(2):
            load_all(k).wait()
        pair_half(pl.ds(0, 2), pair_recv.at[0]).wait_recv()
        shape = acc.shape[1:]
        first = fold(red[0], c_buf[0])
        second = fold(red[1], c_buf[1])
        acc[0] = first.reshape(shape)
        acc[1] = second.reshape(shape)
        part[0] = (first * factor).astype(jnp.bfloat16).reshape(shape)
        part[1] = (second * factor).astype(jnp.bfloat16).reshape(shape)

    def project_last():
        load_all(2).wait()
        pair_half(pl.ds(2, 1), pair_recv.at[1]).wait_recv()
        half = tokens // 2
        total = fold(red[2, :half, :], c_buf[2, :half, :])
        total = total + fold(red[2, half:, :], c_buf[2, half:, :])
        acc[2] = total.reshape(acc.shape[1:])
        part[2] = (total * factor).astype(jnp.bfloat16).reshape(acc.shape[1:])

    with jax.named_scope("barrier"):
        pl.semaphore_wait(barrier, size - 1 + groups - 1)
    stage_0()
    with jax.named_scope("compute0"):
        for k in range(2):
            base_copies[k].wait()
        for tile in range(tiles):
            reduce_pair(tile)
    with jax.named_scope("compute2"):
        base_copies[2].wait()
        for tile in range(tiles):
            reduce_last(tile)
    stage_1()
    with jax.named_scope("project0"):
        project_pair()
        send_parts(0)
        send_parts(1)
    with jax.named_scope("project2"):
        project_last()
        send_parts(2)
    stage_far(1)
    stage_on(0)
    with jax.named_scope("pass0"):
        pass_parts((0, 1))
    with jax.named_scope("pass2"):
        pass_parts((2,))
    stage_far(2)
    for copy in firsts[3:]:
        copy.wait()
    def total_copy(j):
        return pltpu.make_async_remote_copy(
            src_ref=totals.at[0],
            dst_ref=totals.at[j],
            send_sem=send_sem.at[6],
            recv_sem=sum_recv.at[1],
            device_id=(lax.rem(me + j, size), mt),
            device_id_type=MESH,
        )

    def sum_copy(j):
        return pltpu.make_async_remote_copy(
            src_ref=sums.at[0],
            dst_ref=sums.at[j],
            send_sem=send_sem.at[7],
            recv_sem=sum_recv.at[0],
            device_id=(me, lax.rem(mt + j, groups)),
            device_id_type=MESH,
        )

    def sums_arrived():
        return all_of(sums.at[pl.ds(1, groups - 1)], 7, sum_recv.at[0])

    def totals_arrived():
        return all_of(totals.at[pl.ds(1, size - 1)], 6, sum_recv.at[1])

    with jax.named_scope("combine0"):
        own_sum = combine((0, 1))
    with jax.named_scope("combine2"):
        sums[0] = own_sum + combine((2,))
    for j in range(1, groups):
        sum_copy(j).start()
    with jax.named_scope("stage2"):
        stage_on(1)
        stage_3()
    with jax.named_scope("dirs1"):
        pass_dirs()
    with jax.named_scope("stage3"):
        stage_on(2)
    with jax.named_scope("sums"):
        sums_arrived().wait_recv()
        total = sums[0]
        for j in range(1, groups):
            total = total + sums[j]
        totals[0] = total
        for j in range(1, size):
            total_copy(j).start()

    with jax.named_scope("dirs2"):
        all_of(got, 4, dir_recv.at[1]).wait_recv()
    with jax.named_scope("stage5"):
        stage_on(3)
    with jax.named_scope("totals"):
        totals_arrived().wait_recv()
        for j in range(1, size):
            total = total + totals[j]
        scale = lax.rsqrt(total / entries + 1.0)
        for k in range(3):
            scale_ref[k] = jnp.broadcast_to(scale[:, k : k + 1], scale_ref.shape[1:])
    with jax.named_scope("stage6"):
        w_arrived(6)

    with jax.named_scope("drain"):
        all_of(all_w.at[pl.ds(0, size - 1)], 0, w_recv.at[0]).wait_send()
        all_of(got, 1, dir_recv.at[1]).wait_send()
        all_of(last, 2, dir_recv.at[0]).wait_send()
        all_of(last, 3, dir_recv.at[0]).wait_send()
        all_of(got, 4, dir_recv.at[1]).wait_send()
        pair_half(pl.ds(0, 3), pair_recv.at[0]).wait_send()
        totals_arrived().wait_send()
        sums_arrived().wait_send()


def exchange(size, groups, x, oc, fc, vc, go, bases, fw, vw, ow, m1, m2):
    tokens, width = x.shape
    rank = bases.shape[2]
    rows, columns = fw.shape
    rank_rows = m1.shape[1]
    tiles = 2
    bf16, f32 = jnp.bfloat16, jnp.float32
    vmem = pl.BlockSpec(memory_space=pltpu.VMEM)
    dma = pltpu.SemaphoreType.DMA
    kernel = functools.partial(
        exchange_kernel,
        size,
        groups,
        float(tokens * size) ** (-0.5),
        float(rank * columns * groups),
    )
    return pl.pallas_call(
        kernel,
        out_shape=(
            pltpu.VMEM((size, 3, rows, columns), bf16),
            pltpu.VMEM((3, SIDE, SIDE, rank_rows, columns), bf16),
            pltpu.VMEM(bases.shape, bf16),
            pltpu.VMEM((3, 8, 512), f32),
            pltpu.VMEM(m1.shape, f32),
            pltpu.VMEM(m2.shape, f32),
            pltpu.VMEM(fw.shape, f32),
            pltpu.VMEM(vw.shape, f32),
            pltpu.VMEM(ow.shape, f32),
        ),
        in_specs=[pl.BlockSpec(memory_space=pltpu.HBM)] * 11,
        out_specs=(vmem,) * 9,
        scratch_shapes=[
            pltpu.VMEM(m1.shape, f32),
            pltpu.VMEM(m2.shape, f32),
            pltpu.VMEM((tokens // 2, width), bf16),
            pltpu.VMEM((tokens // 2, width), bf16),
            pltpu.VMEM((3, tokens, columns), bf16),
            pltpu.VMEM((3, tokens, rank), bf16),
            pltpu.VMEM((3, SIDE, SIDE, rank_rows, columns), f32),
            pltpu.VMEM((3, SIDE, SIDE, rank_rows, columns), bf16),
            pltpu.VMEM((3, 2, SIDE - 1, SIDE, rank_rows, columns // 2), bf16),
            pltpu.VMEM((3, 2, SIDE, rank_rows, columns // 2), f32),
            pltpu.VMEM((3, 2, SIDE, rank_rows, columns // 2), bf16),
            pltpu.VMEM((3, 2, SIDE - 1, rank_rows, columns // 2), bf16),
            pltpu.VMEM((groups, 1, 128), f32),
            pltpu.VMEM((size, 1, 128), f32),
            dma((5,)),
            dma((2, tiles)),
            dma((3,)),
            dma((3,)),
            dma((2,)),
            dma((8,)),
            dma((7,)),
            dma((2, 2)),
            dma((2,)),
            dma((2,)),
        ],
        compiler_params=pltpu.CompilerParams(
            collective_id=0, has_side_effects=True, vmem_limit_bytes=52 * 1024 * 1024
        ),
    )(x, oc, fc, vc, go, bases, fw, vw, ow, m1, m2)


def finish_kernel(
    scale_ref,
    dirs_ref,
    all_w,
    bases_ref,
    fw_ref,
    vw_ref,
    ow_ref,
    n1_ref,
    n2_ref,
    new_f,
    new_v,
    new_o,
    copy_f,
    copy_v,
    copy_o,
    n1_out,
    n2_out,
    step_f,
    step_v,
    step_o,
    cf_buf,
    cv_buf,
    co_buf,
    down_buf,
    across_buf,
    tile_sem,
    small_sem,
):
    tiles = 4
    rows = cf_buf.shape[0] // tiles
    own = fw_ref.shape[0]
    owners = rows // own

    def put(src, dst, sem):
        pltpu.make_async_copy(src, dst, sem).start()

    put(n1_ref, n1_out, small_sem.at[0])
    put(n2_ref, n2_out, small_sem.at[1])

    def direction(k):
        return dirs_ref[k].reshape(bases_ref.shape[2], down_buf.shape[2])

    def down(at, k):
        step = jnp.dot(bases_ref[k, at, :], direction(k), preferred_element_type=jnp.float32)
        return step * scale_ref[k, 0:1, : step.shape[1]]

    def across(at):
        step = lax.dot_general(
            direction(2),
            bases_ref[2, at, :],
            (((0,), (1,)), ((), ())),
            preferred_element_type=jnp.float32,
        )
        return step * scale_ref[2, 0:1, : step.shape[1]]

    for tile in range(tiles):
        at = pl.ds(tile * rows, rows)
        owned = pl.ds(tile * owners, owners)
        for k, buf, out in ((0, cf_buf, copy_f), (1, cv_buf, copy_v)):
            old = all_w[owned, k].reshape(rows, cf_buf.shape[1])
            value = old.astype(jnp.float32) - 0.01 * down(at, k)
            buf[at, :] = value.astype(jnp.bfloat16)
            put(buf.at[at, :], out.at[at, :], tile_sem.at[k])
        step = across(at)
        for i in range(owners):
            lanes = pl.ds(tile * rows + i * own, own)
            for j in range(2):
                old = all_w[tile * owners + i, 2, :, j * own : (j + 1) * own]
                value = old.astype(jnp.float32) - 0.01 * step[
                    j * own : (j + 1) * own, i * own : (i + 1) * own
                ]
                co_buf[pl.ds(j * own, own), lanes] = value.astype(jnp.bfloat16)
        put(co_buf.at[:, at], copy_o.at[:, at], tile_sem.at[2])

    me = pl.ds(pl.multiple_of(lax.axis_index("fs") * own, own), own)
    for k, weight, new, out in ((0, fw_ref, new_f, step_f), (1, vw_ref, new_v, step_v)):
        step = down(me, k)
        down_buf[2 * k] = step
        put(down_buf.at[2 * k], out, small_sem.at[2])
        down_buf[2 * k + 1] = weight[...] - 0.01 * step
        put(down_buf.at[2 * k + 1], new, small_sem.at[2])
    step = across(me)
    across_buf[0] = step
    put(across_buf.at[0], step_o, small_sem.at[3])
    across_buf[1] = ow_ref[...] - 0.01 * step
    put(across_buf.at[1], new_o, small_sem.at[3])

    for i, buf, out in ((0, cf_buf, copy_f), (1, cv_buf, copy_v), (2, co_buf, copy_o)):
        pltpu.make_async_copy(buf, out, tile_sem.at[i]).wait()
    pltpu.make_async_copy(n1_ref, n1_out, small_sem.at[0]).wait()
    pltpu.make_async_copy(n2_ref, n2_out, small_sem.at[1]).wait()
    pltpu.make_async_copy(down_buf, down_buf, small_sem.at[2]).wait()
    pltpu.make_async_copy(across_buf, across_buf, small_sem.at[3]).wait()


def finish(all_w, dirs, bases, scales, one, two, fw, vw, ow):
    size, _, rows, columns = all_w.shape
    depth = size * rows
    rank = bases.shape[2]
    bf16, f32 = jnp.bfloat16, jnp.float32
    dma = pltpu.SemaphoreType.DMA
    tall = jax.ShapeDtypeStruct((depth, columns), bf16)
    wide = jax.ShapeDtypeStruct((columns, depth), bf16)
    down = jax.ShapeDtypeStruct((rows, columns), f32)
    across = jax.ShapeDtypeStruct((columns, rows), f32)
    small = jax.ShapeDtypeStruct(one.shape, f32)
    return pl.pallas_call(
        finish_kernel,
        out_shape=(down, down, across, tall, tall, wide, small, small, down, down, across),
        in_specs=[pl.BlockSpec(memory_space=pltpu.VMEM)] * 9,
        out_specs=(pl.BlockSpec(memory_space=pltpu.HBM),) * 11,
        scratch_shapes=[
            pltpu.VMEM(tall.shape, bf16),
            pltpu.VMEM(tall.shape, bf16),
            pltpu.VMEM(wide.shape, bf16),
            pltpu.VMEM((4,) + down.shape, f32),
            pltpu.VMEM((2,) + across.shape, f32),
            dma((3,)),
            dma((4,)),
        ],
        compiler_params=pltpu.CompilerParams(vmem_limit_bytes=24 * 1024 * 1024),
        cost_estimate=pl.CostEstimate(
            flops=6 * depth * rank * columns, bytes_accessed=8 * depth * columns, transcendentals=0
        ),
    )(scales, dirs, all_w, bases, fw, vw, ow, one, two)


def on_device(
    normed_input,
    forget_cot,
    value_cot,
    gated_output,
    output_cot,
    forget_weight,
    value_weight,
    out_weight,
    bases,
    first_moment,
    second_moment,
):
    size, groups = lax.axis_size("fs"), lax.axis_size("tp")
    held = exchange(
        size,
        groups,
        normed_input,
        output_cot,
        forget_cot,
        value_cot,
        gated_output,
        bases,
        forget_weight,
        value_weight,
        out_weight,
        first_moment.transpose(1, 0, 2),
        second_moment.transpose(1, 0, 2),
    )
    outs = finish(*held)
    return (
        *outs[:6],
        outs[6].transpose(1, 0, 2),
        outs[7].transpose(1, 0, 2),
        *outs[8:],
    )


def solution(mesh):
    placed = (
        P("fs", None),
        P("fs", "tp"),
        P("fs", "tp"),
        P("fs", "tp"),
        P("fs", None),
        P("fs", "tp"),
        P("fs", "tp"),
        P("tp", "fs"),
        P(),
        P("fs", None, "tp"),
        P("fs", None, "tp"),
    )
    return jax.shard_map(
        on_device,
        mesh=mesh,
        in_specs=placed,
        out_specs=(
            P("fs", "tp"),
            P("fs", "tp"),
            P("tp", "fs"),
            P(None, "tp"),
            P(None, "tp"),
            P("tp", None),
            P("fs", None, "tp"),
            P("fs", None, "tp"),
            P("fs", "tp"),
            P("fs", "tp"),
            P("tp", "fs"),
        ),
        check_vma=False,
    )
```

```python
import functools

import jax
import jax.numpy as jnp
from jax import lax
from jax.experimental import pallas as pl
from jax.experimental.pallas import tpu as pltpu
from jax.sharding import PartitionSpec as P

MESH = pl.DeviceIdType.MESH
SIDE = 4
STEPS = (1, -1)
OFFSETS = (0, -1, 1, 2)


def exchange_kernel(
    size,
    groups,
    factor,
    entries,
    x_hbm,
    oc_hbm,
    fc_hbm,
    vc_hbm,
    go_hbm,
    bases_hbm,
    fw_hbm,
    vw_hbm,
    ow_hbm,
    m1_hbm,
    m2_hbm,
    all_w,
    dirs,
    b_buf,
    scale_ref,
    n1_ref,
    n2_ref,
    fw_ref,
    vw_ref,
    ow_ref,
    m1_ref,
    m2_ref,
    x_buf,
    oc_buf,
    c_buf,
    red,
    acc,
    part,
    got,
    held,
    mid,
    last,
    sums,
    totals,
    first_sem,
    load_sem,
    cot_sem,
    base_sem,
    pair_recv,
    send_sem,
    w_recv,
    part_recv,
    dir_recv,
    sum_recv,
    near_sem,
    across_sem,
    plane_sem,
):
    me = lax.axis_index("fs")
    mt = lax.axis_index("tp")
    z = lax.div(me, SIDE)
    x = lax.rem(me, SIDE)
    core = lax.rem(mt, 2)
    partner = mt + 1 - 2 * core
    tiles = load_sem.shape[1]
    tokens = c_buf.shape[1]
    rows_t = x_buf.shape[0] // tiles
    first_row = core * x_buf.shape[0]
    rank_rows = m1_ref.shape[1]
    columns = m1_ref.shape[2]
    own = fw_ref.shape[0]
    half_rows = own // 2

    firsts = [
        pltpu.make_async_copy(src, dst, first_sem.at[i])
        for i, (src, dst) in enumerate(
            (
                (fw_hbm, fw_ref),
                (vw_hbm, vw_ref),
                (ow_hbm, ow_ref),
                (m1_hbm, m1_ref),
                (m2_hbm, m2_ref),
            )
        )
    ]
    for copy in firsts[:3]:
        copy.start()
    base_copies = [
        pltpu.make_async_copy(bases_hbm.at[k], b_buf.at[k], base_sem.at[k]) for k in range(3)
    ]

    def tile_rows(tile):
        return pl.ds(pl.multiple_of(first_row + tile * rows_t, rows_t), rows_t)

    def load(which, src, dst, tile):
        held = pl.ds(tile * rows_t, rows_t)
        return pltpu.make_async_copy(
            src.at[tile_rows(tile), :], dst.at[held, :], load_sem.at[which, tile]
        )

    def load_all(k):
        return pltpu.make_async_copy((fc_hbm, vc_hbm, go_hbm)[k], c_buf.at[k], cot_sem.at[k])

    streams = ((x_hbm, x_buf), (oc_hbm, oc_buf))
    base_copies[0].start()
    base_copies[1].start()
    load(0, *streams[0], 0).start()

    def ahead(dz, dx):
        return lax.rem(z + dz, SIDE) * SIDE + lax.rem(x + dx, SIDE)

    def along_y(step):
        return lax.rem(mt + 2 * step, groups)

    barrier = pltpu.get_barrier_semaphore()
    around = [(ahead(0, 1), mt), (ahead(0, 3), mt), (ahead(1, 0), mt), (ahead(3, 0), mt)]
    around += [(me, along_y(1)), (me, along_y(3)), (me, partner)]
    for place in around:
        pl.semaphore_signal(barrier, inc=1, device_id=place, device_id_type=MESH)
    for copy in firsts[:3]:
        copy.wait()
    all_w[me, 0] = fw_ref[...].astype(jnp.bfloat16)
    all_w[me, 1] = vw_ref[...].astype(jnp.bfloat16)
    all_w[me, 2, :, :own] = ow_ref[:own, :].astype(jnp.bfloat16)
    all_w[me, 2, :, own:] = ow_ref[own:, :].astype(jnp.bfloat16)

    def node(h, a, b):
        dz, dx = (b, a) if h == 0 else (a, b)
        return lax.rem(z + dz + SIDE, SIDE) * SIDE + lax.rem(x + dx + SIDE, SIDE)

    def w_copy(h, slot, owner, quarter, dest):
        start, count = h * half_rows, half_rows
        if quarter is not None:
            count = half_rows // 2
            start = start + quarter * count
        view = all_w.at[owner, :, pl.ds(start, count), :]
        return pltpu.make_async_remote_copy(
            src_ref=view,
            dst_ref=view,
            send_sem=send_sem.at[0],
            recv_sem=w_recv.at[slot],
            device_id=(dest, mt),
            device_id_type=MESH,
        )

    def near(h, s):
        return w_copy(h, 0, me, None, node(h, STEPS[s], 0))

    def near_on(h, s):
        return w_copy(h, 1, node(h, -STEPS[s], 0), s, node(h, STEPS[s], 0))

    def far(h, i, s):
        return w_copy(h, 2 + i, node(h, OFFSETS[i], 0), None, node(h, 0, STEPS[s]))

    def far_on(h, i, s):
        return w_copy(h, 6, node(h, OFFSETS[i], -STEPS[s]), s, node(h, 0, STEPS[s]))

    def all_of(view, send, recv, to=None):
        return pltpu.make_async_remote_copy(
            src_ref=view,
            dst_ref=view,
            send_sem=send_sem.at[send],
            recv_sem=recv,
            device_id=(node(0, 1, 0), mt) if to is None else to,
            device_id_type=MESH,
        )

    def w_arrived(slot):
        count = (2, 1, 2, 2, 2, 2, 4)[slot]
        all_of(all_w.at[pl.ds(0, count)], 0, w_recv.at[slot]).wait_recv()

    def each(start):
        for h in range(2):
            for s in range(2):
                start(h, s).start()

    def stage_0():
        each(near)
        stage_far(0)

    def stage_1():
        w_arrived(0)
        each(near_on)

    def stage_far(i):
        each(lambda h, s: far(h, i, s))

    def stage_on(i):
        w_arrived(2 + i)
        each(lambda h, s: far_on(h, i, s))

    def stage_3():
        w_arrived(1)
        stage_far(3)

    half_cols = columns // 2

    def cut(h):
        return pl.ds(h * half_cols, half_cols)

    def line(h, second, j):
        first_axis = (h == 0) != second
        return (
            z * SIDE + lax.rem(x + j, SIDE) if first_axis else lax.rem(z + j, SIDE) * SIDE + x
        )

    def blocks(ref, k, h, j):
        if h == 0:
            return ref.at[k, :, lax.rem(x + j, SIDE), :, cut(h)]
        return ref.at[k, lax.rem(z + j, SIDE), :, :, cut(h)]

    def move(src, dst, send, recv, dest):
        return pltpu.make_async_remote_copy(
            src_ref=src,
            dst_ref=dst,
            send_sem=send_sem.at[send],
            recv_sem=recv,
            device_id=(dest, mt),
            device_id_type=MESH,
        )

    def part_first(k, h, j):
        return move(
            blocks(part, k, h, j), got.at[k, h, j - 1], 1, part_recv.at[0, k // 2], line(h, False, j)
        )

    def part_second(k, h, j):
        place = lax.rem((z if h == 0 else x) + j, SIDE)
        return move(
            mid.at[k, h, place], last.at[k, h, j - 1], 2, part_recv.at[1, k // 2], line(h, True, j)
        )

    def dir_first(k, h, j):
        view = dirs.at[k, z, x, :, cut(h)]
        return move(view, view, 3, dir_recv.at[0], line(h, False, j))

    def dir_second(k, h, j):
        view = dirs.at[k, z, :, :, cut(h)] if h == 0 else dirs.at[k, :, x, :, cut(h)]
        return move(view, view, 4, dir_recv.at[1], line(h, True, j))

    def group_of(ref, ks):
        return ref.at[pl.ds(ks[0], len(ks))]

    ALL = [(h, j) for h in range(2) for j in range(1, SIDE)]

    def send_parts(k):
        for h, j in ALL:
            part_first(k, h, j).start()

    def pass_parts(ks):
        all_of(group_of(got, ks), 1, part_recv.at[0, ks[0] // 2]).wait_recv()
        for k in ks:
            for h in range(2):
                own_part = acc[k, :, x, :, cut(h)] if h == 0 else acc[k, z, :, :, cut(h)]
                total = own_part * factor
                for j in range(1, SIDE):
                    total = total + got[k, h, j - 1].astype(jnp.float32)
                held[k, h] = total
                mid[k, h] = total.astype(jnp.bfloat16)
                for j in range(1, SIDE):
                    part_second(k, h, j).start()

    lane = lax.broadcasted_iota(jnp.int32, sums.shape[1:], 1)

    def combine(ks):
        all_of(group_of(last, ks), 2, part_recv.at[1, ks[0] // 2]).wait_recv()
        return sum(update(k) for k in ks)

    def update(k):
        square = jnp.zeros((rank_rows, half_cols), jnp.float32)
        for h in range(2):
            projected = held[k, h, z if h == 0 else x]
            for j in range(1, SIDE):
                projected = projected + last[k, h, j - 1].astype(jnp.float32)
            one = 0.9 * m1_ref[k, :, cut(h)] + 0.1 * projected
            two = 0.9 * m2_ref[k, :, cut(h)] + 0.1 * projected * projected
            n1_ref[k, :, cut(h)] = one
            n2_ref[k, :, cut(h)] = two
            rounded = (one / (jnp.sqrt(two) + 1e-08)).astype(jnp.bfloat16)
            dirs[k, z, x, :, cut(h)] = rounded
            for j in range(1, SIDE):
                dir_first(k, h, j).start()
            value = rounded.astype(jnp.float32)
            square = square + value * value
        return jnp.where(lane == k, jnp.sum(square), 0.0)

    def pass_dirs():
        all_of(last, 3, dir_recv.at[0]).wait_recv()
        for k in range(3):
            for h, j in ALL:
                dir_second(k, h, j).start()

    def pair_copy(k, tile):
        view = red.at[k, tile_rows(tile), :]
        return pltpu.make_async_remote_copy(
            src_ref=view,
            dst_ref=view,
            send_sem=send_sem.at[5],
            recv_sem=pair_recv.at[k // 2],
            device_id=(me, partner),
            device_id_type=MESH,
        )

    def pair_half(ks, recv):
        view = red.at[ks, pl.ds(0, tokens // 2), :]
        return all_of(view, 5, recv, (me, partner))

    def reduce_pair(tile):
        load(0, *streams[0], tile).wait()
        rows = x_buf[pl.ds(tile * rows_t, rows_t), :]
        first = jnp.dot(rows, b_buf[0], preferred_element_type=jnp.float32)
        second = jnp.dot(rows, b_buf[1], preferred_element_type=jnp.float32)
        red[0, tile_rows(tile), :] = first.astype(jnp.bfloat16)
        red[1, tile_rows(tile), :] = second.astype(jnp.bfloat16)
        for k in range(2):
            pair_copy(k, tile).start()

    def reduce_last(tile):
        load(1, *streams[1], tile).wait()
        half = rows_t // 2
        upper, lower = pl.ds(tile * rows_t, half), pl.ds(tile * rows_t + half, half)
        first = jnp.dot(oc_buf[upper, :], b_buf[2], preferred_element_type=jnp.float32)
        second = jnp.dot(oc_buf[lower, :], b_buf[2], preferred_element_type=jnp.float32)
        both = jnp.concatenate([first, second], axis=0)
        red[2, tile_rows(tile), :] = both.astype(jnp.bfloat16)
        pair_copy(2, tile).start()

    def fold(left, right):
        return lax.dot_general(
            left, right, (((0,), (0,)), ((), ())), preferred_element_type=jnp.float32
        )

    def project_pair():
        for k in range(2):
            load_all(k).wait()
        pair_half(pl.ds(0, 2), pair_recv.at[0]).wait_recv()
        shape = acc.shape[1:]
        first = fold(red[0], c_buf[0])
        second = fold(red[1], c_buf[1])
        acc[0] = first.reshape(shape)
        acc[1] = second.reshape(shape)
        part[0] = (first * factor).astype(jnp.bfloat16).reshape(shape)
        part[1] = (second * factor).astype(jnp.bfloat16).reshape(shape)

    def project_last():
        load_all(2).wait()
        pair_half(pl.ds(2, 1), pair_recv.at[1]).wait_recv()
        half = tokens // 2
        total = fold(red[2, :half, :], c_buf[2, :half, :])
        total = total + fold(red[2, half:, :], c_buf[2, half:, :])
        acc[2] = total.reshape(acc.shape[1:])
        part[2] = (total * factor).astype(jnp.bfloat16).reshape(acc.shape[1:])

    for tile in range(1, tiles):
        load(0, *streams[0], tile).start()
    base_copies[2].start()
    for tile in range(tiles):
        load(1, *streams[1], tile).start()
    for k in range(3):
        load_all(k).start()
    for copy in firsts[3:]:
        copy.start()
    with jax.named_scope("barrier"):
        pl.semaphore_wait(barrier, len(around))
    next_to = [around[0], around[2], around[4], around[5]]
    for place in next_to:
        pl.semaphore_signal(near_sem, inc=1, device_id=place, device_id_type=MESH)
    stage_0()
    with jax.named_scope("compute0"):
        for k in range(2):
            base_copies[k].wait()
        for tile in range(tiles):
            reduce_pair(tile)
    with jax.named_scope("compute2"):
        base_copies[2].wait()
        for tile in range(tiles):
            reduce_last(tile)
    stage_1()
    with jax.named_scope("project0"):
        project_pair()
        pl.semaphore_wait(near_sem, len(next_to))
        pl.semaphore_signal(
            across_sem, inc=1, device_id=(me, along_y(2)), device_id_type=MESH
        )
        for step in range(1, SIDE):
            pl.semaphore_signal(
                plane_sem, inc=1, device_id=(ahead(0, step), mt), device_id_type=MESH
            )
        send_parts(0)
        send_parts(1)
    with jax.named_scope("project2"):
        project_last()
        send_parts(2)
    stage_far(1)
    stage_on(0)
    with jax.named_scope("pass0"):
        pass_parts((0, 1))
    with jax.named_scope("pass2"):
        pass_parts((2,))
    stage_far(2)
    for copy in firsts[3:]:
        copy.wait()
    def total_copy(j):
        return pltpu.make_async_remote_copy(
            src_ref=totals.at[0],
            dst_ref=totals.at[j],
            send_sem=send_sem.at[6],
            recv_sem=sum_recv.at[1],
            device_id=(lax.rem(me + j, size), mt),
            device_id_type=MESH,
        )

    def sum_copy(j):
        return pltpu.make_async_remote_copy(
            src_ref=sums.at[0],
            dst_ref=sums.at[j],
            send_sem=send_sem.at[7],
            recv_sem=sum_recv.at[0],
            device_id=(me, lax.rem(mt + j, groups)),
            device_id_type=MESH,
        )

    def sums_arrived():
        return all_of(sums.at[pl.ds(1, groups - 1)], 7, sum_recv.at[0])

    def totals_arrived():
        return all_of(totals.at[pl.ds(1, size - 1)], 6, sum_recv.at[1])

    with jax.named_scope("combine0"):
        own_sum = combine((0, 1))
    with jax.named_scope("combine2"):
        sums[0] = own_sum + combine((2,))
    pl.semaphore_wait(across_sem, 1)
    for j in range(1, groups):
        sum_copy(j).start()
    with jax.named_scope("stage2"):
        stage_on(1)
        stage_3()
    with jax.named_scope("dirs1"):
        pass_dirs()
    with jax.named_scope("sums"):
        sums_arrived().wait_recv()
        total = sums[0]
        for j in range(1, groups):
            total = total + sums[j]
        totals[0] = total
        pl.semaphore_wait(plane_sem, SIDE - 1)
        for j in range(1, size):
            total_copy(j).start()

    with jax.named_scope("stage3"):
        stage_on(2)
    with jax.named_scope("stage5"):
        stage_on(3)
    with jax.named_scope("dirs2"):
        all_of(got, 4, dir_recv.at[1]).wait_recv()
    with jax.named_scope("totals"):
        totals_arrived().wait_recv()
        for j in range(1, size):
            total = total + totals[j]
        scale = lax.rsqrt(total / entries + 1.0)
        for k in range(3):
            scale_ref[k] = jnp.broadcast_to(scale[:, k : k + 1], scale_ref.shape[1:])
    with jax.named_scope("stage6"):
        w_arrived(6)

    with jax.named_scope("drain"):
        all_of(all_w.at[pl.ds(0, size - 1)], 0, w_recv.at[0]).wait_send()
        all_of(got, 1, dir_recv.at[1]).wait_send()
        all_of(last, 2, dir_recv.at[0]).wait_send()
        all_of(last, 3, dir_recv.at[0]).wait_send()
        all_of(got, 4, dir_recv.at[1]).wait_send()
        pair_half(pl.ds(0, 3), pair_recv.at[0]).wait_send()
        totals_arrived().wait_send()
        sums_arrived().wait_send()


def exchange(size, groups, x, oc, fc, vc, go, bases, fw, vw, ow, m1, m2):
    tokens, width = x.shape
    rank = bases.shape[2]
    rows, columns = fw.shape
    rank_rows = m1.shape[1]
    tiles = 2
    bf16, f32 = jnp.bfloat16, jnp.float32
    vmem = pl.BlockSpec(memory_space=pltpu.VMEM)
    dma = pltpu.SemaphoreType.DMA
    kernel = functools.partial(
        exchange_kernel,
        size,
        groups,
        float(tokens * size) ** (-0.5),
        float(rank * columns * groups),
    )
    return pl.pallas_call(
        kernel,
        out_shape=(
            pltpu.VMEM((size, 3, rows, columns), bf16),
            pltpu.VMEM((3, SIDE, SIDE, rank_rows, columns), bf16),
            pltpu.VMEM(bases.shape, bf16),
            pltpu.VMEM((3, 8, 512), f32),
            pltpu.VMEM(m1.shape, f32),
            pltpu.VMEM(m2.shape, f32),
            pltpu.VMEM(fw.shape, f32),
            pltpu.VMEM(vw.shape, f32),
            pltpu.VMEM(ow.shape, f32),
        ),
        in_specs=[pl.BlockSpec(memory_space=pltpu.HBM)] * 11,
        out_specs=(vmem,) * 9,
        scratch_shapes=[
            pltpu.VMEM(m1.shape, f32),
            pltpu.VMEM(m2.shape, f32),
            pltpu.VMEM((tokens // 2, width), bf16),
            pltpu.VMEM((tokens // 2, width), bf16),
            pltpu.VMEM((3, tokens, columns), bf16),
            pltpu.VMEM((3, tokens, rank), bf16),
            pltpu.VMEM((3, SIDE, SIDE, rank_rows, columns), f32),
            pltpu.VMEM((3, SIDE, SIDE, rank_rows, columns), bf16),
            pltpu.VMEM((3, 2, SIDE - 1, SIDE, rank_rows, columns // 2), bf16),
            pltpu.VMEM((3, 2, SIDE, rank_rows, columns // 2), f32),
            pltpu.VMEM((3, 2, SIDE, rank_rows, columns // 2), bf16),
            pltpu.VMEM((3, 2, SIDE - 1, rank_rows, columns // 2), bf16),
            pltpu.VMEM((groups, 1, 128), f32),
            pltpu.VMEM((size, 1, 128), f32),
            dma((5,)),
            dma((2, tiles)),
            dma((3,)),
            dma((3,)),
            dma((2,)),
            dma((8,)),
            dma((7,)),
            dma((2, 2)),
            dma((2,)),
            dma((2,)),
            pltpu.SemaphoreType.REGULAR,
            pltpu.SemaphoreType.REGULAR,
            pltpu.SemaphoreType.REGULAR,
        ],
        compiler_params=pltpu.CompilerParams(
            collective_id=0, has_side_effects=True, vmem_limit_bytes=52 * 1024 * 1024
        ),
    )(x, oc, fc, vc, go, bases, fw, vw, ow, m1, m2)


def finish_kernel(
    scale_ref,
    dirs_ref,
    all_w,
    bases_ref,
    fw_ref,
    vw_ref,
    ow_ref,
    n1_ref,
    n2_ref,
    new_f,
    new_v,
    new_o,
    copy_f,
    copy_v,
    copy_o,
    n1_out,
    n2_out,
    step_f,
    step_v,
    step_o,
    cf_buf,
    cv_buf,
    co_buf,
    down_buf,
    across_buf,
    tile_sem,
    small_sem,
):
    tiles = 4
    rows = cf_buf.shape[0] // tiles
    own = fw_ref.shape[0]
    owners = rows // own

    def put(src, dst, sem):
        pltpu.make_async_copy(src, dst, sem).start()

    put(n1_ref, n1_out, small_sem.at[0])
    put(n2_ref, n2_out, small_sem.at[1])

    def direction(k):
        return dirs_ref[k].reshape(bases_ref.shape[2], down_buf.shape[2])

    def down(at, k):
        step = jnp.dot(bases_ref[k, at, :], direction(k), preferred_element_type=jnp.float32)
        return step * scale_ref[k, 0:1, : step.shape[1]]

    def across(at):
        step = lax.dot_general(
            direction(2),
            bases_ref[2, at, :],
            (((0,), (1,)), ((), ())),
            preferred_element_type=jnp.float32,
        )
        return step * scale_ref[2, 0:1, : step.shape[1]]

    for tile in range(tiles):
        at = pl.ds(tile * rows, rows)
        owned = pl.ds(tile * owners, owners)
        for k, buf, out in ((0, cf_buf, copy_f), (1, cv_buf, copy_v)):
            old = all_w[owned, k].reshape(rows, cf_buf.shape[1])
            value = old.astype(jnp.float32) - 0.01 * down(at, k)
            buf[at, :] = value.astype(jnp.bfloat16)
            put(buf.at[at, :], out.at[at, :], tile_sem.at[k])
        step = across(at)
        for i in range(owners):
            lanes = pl.ds(tile * rows + i * own, own)
            for j in range(2):
                old = all_w[tile * owners + i, 2, :, j * own : (j + 1) * own]
                value = old.astype(jnp.float32) - 0.01 * step[
                    j * own : (j + 1) * own, i * own : (i + 1) * own
                ]
                co_buf[pl.ds(j * own, own), lanes] = value.astype(jnp.bfloat16)
        put(co_buf.at[:, at], copy_o.at[:, at], tile_sem.at[2])

    me = pl.ds(pl.multiple_of(lax.axis_index("fs") * own, own), own)
    for k, weight, new, out in ((0, fw_ref, new_f, step_f), (1, vw_ref, new_v, step_v)):
        step = down(me, k)
        down_buf[2 * k] = step
        put(down_buf.at[2 * k], out, small_sem.at[2])
        down_buf[2 * k + 1] = weight[...] - 0.01 * step
        put(down_buf.at[2 * k + 1], new, small_sem.at[2])
    step = across(me)
    across_buf[0] = step
    put(across_buf.at[0], step_o, small_sem.at[3])
    across_buf[1] = ow_ref[...] - 0.01 * step
    put(across_buf.at[1], new_o, small_sem.at[3])

    for i, buf, out in ((0, cf_buf, copy_f), (1, cv_buf, copy_v), (2, co_buf, copy_o)):
        pltpu.make_async_copy(buf, out, tile_sem.at[i]).wait()
    pltpu.make_async_copy(n1_ref, n1_out, small_sem.at[0]).wait()
    pltpu.make_async_copy(n2_ref, n2_out, small_sem.at[1]).wait()
    pltpu.make_async_copy(down_buf, down_buf, small_sem.at[2]).wait()
    pltpu.make_async_copy(across_buf, across_buf, small_sem.at[3]).wait()


def finish(all_w, dirs, bases, scales, one, two, fw, vw, ow):
    size, _, rows, columns = all_w.shape
    depth = size * rows
    rank = bases.shape[2]
    bf16, f32 = jnp.bfloat16, jnp.float32
    dma = pltpu.SemaphoreType.DMA
    tall = jax.ShapeDtypeStruct((depth, columns), bf16)
    wide = jax.ShapeDtypeStruct((columns, depth), bf16)
    down = jax.ShapeDtypeStruct((rows, columns), f32)
    across = jax.ShapeDtypeStruct((columns, rows), f32)
    small = jax.ShapeDtypeStruct(one.shape, f32)
    return pl.pallas_call(
        finish_kernel,
        out_shape=(down, down, across, tall, tall, wide, small, small, down, down, across),
        in_specs=[pl.BlockSpec(memory_space=pltpu.VMEM)] * 9,
        out_specs=(pl.BlockSpec(memory_space=pltpu.HBM),) * 11,
        scratch_shapes=[
            pltpu.VMEM(tall.shape, bf16),
            pltpu.VMEM(tall.shape, bf16),
            pltpu.VMEM(wide.shape, bf16),
            pltpu.VMEM((4,) + down.shape, f32),
            pltpu.VMEM((2,) + across.shape, f32),
            dma((3,)),
            dma((4,)),
        ],
        compiler_params=pltpu.CompilerParams(vmem_limit_bytes=24 * 1024 * 1024),
        cost_estimate=pl.CostEstimate(
            flops=6 * depth * rank * columns, bytes_accessed=8 * depth * columns, transcendentals=0
        ),
    )(scales, dirs, all_w, bases, fw, vw, ow, one, two)


def on_device(
    normed_input,
    forget_cot,
    value_cot,
    gated_output,
    output_cot,
    forget_weight,
    value_weight,
    out_weight,
    bases,
    first_moment,
    second_moment,
):
    size, groups = lax.axis_size("fs"), lax.axis_size("tp")
    held = exchange(
        size,
        groups,
        normed_input,
        output_cot,
        forget_cot,
        value_cot,
        gated_output,
        bases,
        forget_weight,
        value_weight,
        out_weight,
        first_moment.transpose(1, 0, 2),
        second_moment.transpose(1, 0, 2),
    )
    outs = finish(*held)
    return (
        *outs[:6],
        outs[6].transpose(1, 0, 2),
        outs[7].transpose(1, 0, 2),
        *outs[8:],
    )


def solution(mesh):
    placed = (
        P("fs", None),
        P("fs", "tp"),
        P("fs", "tp"),
        P("fs", "tp"),
        P("fs", None),
        P("fs", "tp"),
        P("fs", "tp"),
        P("tp", "fs"),
        P(),
        P("fs", None, "tp"),
        P("fs", None, "tp"),
    )
    return jax.shard_map(
        on_device,
        mesh=mesh,
        in_specs=placed,
        out_specs=(
            P("fs", "tp"),
            P("fs", "tp"),
            P("tp", "fs"),
            P(None, "tp"),
            P(None, "tp"),
            P("tp", None),
            P("fs", None, "tp"),
            P("fs", None, "tp"),
            P("fs", "tp"),
            P("fs", "tp"),
            P("tp", "fs"),
        ),
        check_vma=False,
    )
```

```python
import functools

import jax
import jax.numpy as jnp
from jax import lax
from jax.experimental import pallas as pl
from jax.experimental.pallas import tpu as pltpu
from jax.sharding import PartitionSpec as P

MESH = pl.DeviceIdType.MESH
SIDE = 4
STEPS = (1, -1)
OFFSETS = (0, -1, 1, 2)


def exchange_kernel(
    size,
    groups,
    factor,
    entries,
    x_hbm,
    oc_hbm,
    fc_hbm,
    vc_hbm,
    go_hbm,
    bases_hbm,
    fw_hbm,
    vw_hbm,
    ow_hbm,
    m1_hbm,
    m2_hbm,
    all_w,
    dirs,
    b_buf,
    scale_ref,
    n1_ref,
    n2_ref,
    fw_ref,
    vw_ref,
    ow_ref,
    m1_ref,
    m2_ref,
    x_buf,
    oc_buf,
    c_buf,
    red,
    acc,
    part,
    got,
    held,
    mid,
    last,
    sums,
    totals,
    first_sem,
    load_sem,
    cot_sem,
    base_sem,
    pair_recv,
    send_sem,
    w_recv,
    part_recv,
    dir_recv,
    sum_recv,
    near_sem,
    across_sem,
    plane_sem,
):
    me = lax.axis_index("fs")
    mt = lax.axis_index("tp")
    z = lax.div(me, SIDE)
    x = lax.rem(me, SIDE)
    core = lax.rem(mt, 2)
    partner = mt + 1 - 2 * core
    tokens = c_buf.shape[1]
    quarter_rows = x_buf.shape[0] // 4
    cuts = (((0, 1), (1, 2), (3, 1)), ((0, 2), (2, 2)))
    first_row = core * x_buf.shape[0]
    rank_rows = m1_ref.shape[1]
    columns = m1_ref.shape[2]
    own = fw_ref.shape[0]
    half_rows = own // 2

    firsts = [
        pltpu.make_async_copy(src, dst, first_sem.at[i])
        for i, (src, dst) in enumerate(
            (
                (fw_hbm, fw_ref),
                (vw_hbm, vw_ref),
                (ow_hbm, ow_ref),
                (m1_hbm, m1_ref),
                (m2_hbm, m2_ref),
            )
        )
    ]
    for copy in firsts[:3]:
        copy.start()
    base_copies = [
        pltpu.make_async_copy(bases_hbm.at[k], b_buf.at[k], base_sem.at[k]) for k in range(3)
    ]

    def tile_rows(which, tile):
        start, count = cuts[which][tile]
        rows = count * quarter_rows
        return pl.ds(pl.multiple_of(first_row + start * quarter_rows, quarter_rows), rows)

    def held_rows(which, tile):
        start, count = cuts[which][tile]
        return pl.ds(start * quarter_rows, count * quarter_rows)

    def load(which, src, dst, tile):
        return pltpu.make_async_copy(
            src.at[tile_rows(which, tile), :],
            dst.at[held_rows(which, tile), :],
            load_sem.at[which, tile],
        )

    def load_all(k):
        return pltpu.make_async_copy((fc_hbm, vc_hbm, go_hbm)[k], c_buf.at[k], cot_sem.at[k])

    streams = ((x_hbm, x_buf), (oc_hbm, oc_buf))
    base_copies[0].start()
    load(0, *streams[0], 0).start()
    base_copies[1].start()

    def ahead(dz, dx):
        return lax.rem(z + dz, SIDE) * SIDE + lax.rem(x + dx, SIDE)

    def along_y(step):
        return lax.rem(mt + 2 * step, groups)

    barrier = pltpu.get_barrier_semaphore()
    around = [(ahead(0, 1), mt), (ahead(0, 3), mt), (ahead(1, 0), mt), (ahead(3, 0), mt)]
    around += [(me, along_y(1)), (me, along_y(3)), (me, partner)]
    for place in around:
        pl.semaphore_signal(barrier, inc=1, device_id=place, device_id_type=MESH)
    for copy in firsts[:3]:
        copy.wait()
    all_w[me, 0] = fw_ref[...].astype(jnp.bfloat16)
    all_w[me, 1] = vw_ref[...].astype(jnp.bfloat16)
    all_w[me, 2, :, :own] = ow_ref[:own, :].astype(jnp.bfloat16)
    all_w[me, 2, :, own:] = ow_ref[own:, :].astype(jnp.bfloat16)

    def node(h, a, b):
        dz, dx = (b, a) if h == 0 else (a, b)
        return lax.rem(z + dz + SIDE, SIDE) * SIDE + lax.rem(x + dx + SIDE, SIDE)

    def w_copy(h, slot, owner, quarter, dest):
        start, count = h * half_rows, half_rows
        if quarter is not None:
            count = half_rows // 2
            start = start + quarter * count
        view = all_w.at[owner, :, pl.ds(start, count), :]
        return pltpu.make_async_remote_copy(
            src_ref=view,
            dst_ref=view,
            send_sem=send_sem.at[0],
            recv_sem=w_recv.at[slot],
            device_id=(dest, mt),
            device_id_type=MESH,
        )

    def near(h, s):
        return w_copy(h, 0, me, None, node(h, STEPS[s], 0))

    def near_on(h, s):
        return w_copy(h, 1, node(h, -STEPS[s], 0), s, node(h, STEPS[s], 0))

    def far(h, i, s):
        return w_copy(h, 2 + i, node(h, OFFSETS[i], 0), None, node(h, 0, STEPS[s]))

    def far_on(h, i, s):
        return w_copy(h, 6, node(h, OFFSETS[i], -STEPS[s]), s, node(h, 0, STEPS[s]))

    def all_of(view, send, recv, to=None):
        return pltpu.make_async_remote_copy(
            src_ref=view,
            dst_ref=view,
            send_sem=send_sem.at[send],
            recv_sem=recv,
            device_id=(node(0, 1, 0), mt) if to is None else to,
            device_id_type=MESH,
        )

    def w_arrived(slot):
        count = (2, 1, 2, 2, 2, 2, 4)[slot]
        all_of(all_w.at[pl.ds(0, count)], 0, w_recv.at[slot]).wait_recv()

    def each(start):
        for h in range(2):
            for s in range(2):
                start(h, s).start()

    def stage_0():
        each(near)
        stage_far(0)

    def stage_1():
        w_arrived(0)
        each(near_on)

    def stage_far(i):
        each(lambda h, s: far(h, i, s))

    def stage_on(i):
        w_arrived(2 + i)
        each(lambda h, s: far_on(h, i, s))

    def stage_3():
        w_arrived(1)
        stage_far(3)

    half_cols = columns // 2

    def cut(h):
        return pl.ds(h * half_cols, half_cols)

    def line(h, second, j):
        first_axis = (h == 0) != second
        return (
            z * SIDE + lax.rem(x + j, SIDE) if first_axis else lax.rem(z + j, SIDE) * SIDE + x
        )

    def blocks(ref, k, h, j):
        if h == 0:
            return ref.at[k, :, lax.rem(x + j, SIDE), :, cut(h)]
        return ref.at[k, lax.rem(z + j, SIDE), :, :, cut(h)]

    def move(src, dst, send, recv, dest):
        return pltpu.make_async_remote_copy(
            src_ref=src,
            dst_ref=dst,
            send_sem=send_sem.at[send],
            recv_sem=recv,
            device_id=(dest, mt),
            device_id_type=MESH,
        )

    def part_first(k, h, j):
        return move(
            blocks(part, k, h, j), got.at[k, h, j - 1], 1, part_recv.at[0, k // 2], line(h, False, j)
        )

    def part_second(k, h, j):
        place = lax.rem((z if h == 0 else x) + j, SIDE)
        return move(
            mid.at[k, h, place], last.at[k, h, j - 1], 2, part_recv.at[1, k // 2], line(h, True, j)
        )

    def dir_first(k, h, j):
        view = dirs.at[k, z, x, :, cut(h)]
        return move(view, view, 3, dir_recv.at[k // 2], line(h, False, j))

    def dir_second(k, h, j):
        view = dirs.at[k, z, :, :, cut(h)] if h == 0 else dirs.at[k, :, x, :, cut(h)]
        return move(view, view, 4, dir_recv.at[2], line(h, True, j))

    def group_of(ref, ks):
        return ref.at[pl.ds(ks[0], len(ks))]

    ALL = [(h, j) for h in range(2) for j in range(1, SIDE)]

    def send_parts(k):
        for h, j in ALL:
            part_first(k, h, j).start()

    def pass_parts(ks):
        all_of(group_of(got, ks), 1, part_recv.at[0, ks[0] // 2]).wait_recv()
        for k in ks:
            for h in range(2):
                own_part = acc[k, :, x, :, cut(h)] if h == 0 else acc[k, z, :, :, cut(h)]
                total = own_part * factor
                for j in range(1, SIDE):
                    total = total + got[k, h, j - 1].astype(jnp.float32)
                held[k, h] = total
                mid[k, h] = total.astype(jnp.bfloat16)
                for j in range(1, SIDE):
                    part_second(k, h, j).start()

    lane = lax.broadcasted_iota(jnp.int32, sums.shape[1:], 1)

    def combine(ks):
        all_of(group_of(last, ks), 2, part_recv.at[1, ks[0] // 2]).wait_recv()
        return sum(update(k) for k in ks)

    def update(k):
        square = jnp.zeros((rank_rows, half_cols), jnp.float32)
        for h in range(2):
            projected = held[k, h, z if h == 0 else x]
            for j in range(1, SIDE):
                projected = projected + last[k, h, j - 1].astype(jnp.float32)
            one = 0.9 * m1_ref[k, :, cut(h)] + 0.1 * projected
            two = 0.9 * m2_ref[k, :, cut(h)] + 0.1 * projected * projected
            n1_ref[k, :, cut(h)] = one
            n2_ref[k, :, cut(h)] = two
            rounded = (one / (jnp.sqrt(two) + 1e-08)).astype(jnp.bfloat16)
            dirs[k, z, x, :, cut(h)] = rounded
            for j in range(1, SIDE):
                dir_first(k, h, j).start()
            value = rounded.astype(jnp.float32)
            square = square + value * value
        return jnp.where(lane == k, jnp.sum(square), 0.0)

    def pass_dirs(ks):
        all_of(group_of(last, ks), 3, dir_recv.at[ks[0] // 2]).wait_recv()
        for k in ks:
            for h, j in ALL:
                dir_second(k, h, j).start()

    def pair_copy(k, tile):
        view = red.at[k, tile_rows(k // 2, tile), :]
        return pltpu.make_async_remote_copy(
            src_ref=view,
            dst_ref=view,
            send_sem=send_sem.at[5],
            recv_sem=pair_recv.at[k // 2],
            device_id=(me, partner),
            device_id_type=MESH,
        )

    def pair_half(ks, recv):
        view = red.at[ks, pl.ds(0, tokens // 2), :]
        return all_of(view, 5, recv, (me, partner))

    def reduce_pair(tile):
        load(0, *streams[0], tile).wait()
        rows = x_buf[held_rows(0, tile), :]
        at = tile_rows(0, tile)
        first = jnp.dot(rows, b_buf[0], preferred_element_type=jnp.float32)
        second = jnp.dot(rows, b_buf[1], preferred_element_type=jnp.float32)
        red[0, at, :] = first.astype(jnp.bfloat16)
        red[1, at, :] = second.astype(jnp.bfloat16)
        for k in range(2):
            pair_copy(k, tile).start()

    def reduce_last(tile):
        load(1, *streams[1], tile).wait()
        start, count = cuts[1][tile]
        half = count * quarter_rows // 2
        upper = pl.ds(start * quarter_rows, half)
        lower = pl.ds(start * quarter_rows + half, half)
        first = jnp.dot(oc_buf[upper, :], b_buf[2], preferred_element_type=jnp.float32)
        second = jnp.dot(oc_buf[lower, :], b_buf[2], preferred_element_type=jnp.float32)
        both = jnp.concatenate([first, second], axis=0)
        red[2, tile_rows(1, tile), :] = both.astype(jnp.bfloat16)
        pair_copy(2, tile).start()

    def fold(left, right):
        return lax.dot_general(
            left, right, (((0,), (0,)), ((), ())), preferred_element_type=jnp.float32
        )

    def project_pair():
        for k in range(2):
            load_all(k).wait()
        pair_half(pl.ds(0, 2), pair_recv.at[0]).wait_recv()
        shape = acc.shape[1:]
        first = fold(red[0], c_buf[0])
        second = fold(red[1], c_buf[1])
        acc[0] = first.reshape(shape)
        acc[1] = second.reshape(shape)
        part[0] = (first * factor).astype(jnp.bfloat16).reshape(shape)
        part[1] = (second * factor).astype(jnp.bfloat16).reshape(shape)

    def project_last():
        load_all(2).wait()
        pair_half(pl.ds(2, 1), pair_recv.at[1]).wait_recv()
        half = tokens // 2
        total = fold(red[2, :half, :], c_buf[2, :half, :])
        total = total + fold(red[2, half:, :], c_buf[2, half:, :])
        acc[2] = total.reshape(acc.shape[1:])
        part[2] = (total * factor).astype(jnp.bfloat16).reshape(acc.shape[1:])

    for tile in range(1, len(cuts[0])):
        load(0, *streams[0], tile).start()
    with jax.named_scope("barrier"):
        pl.semaphore_wait(barrier, len(around))
    next_to = [around[0], around[2], around[4], around[5]]
    for place in next_to:
        pl.semaphore_signal(near_sem, inc=1, device_id=place, device_id_type=MESH)
    stage_0()
    with jax.named_scope("compute0"):
        for k in range(2):
            base_copies[k].wait()
        for tile in range(len(cuts[0])):
            reduce_pair(tile)
            if tile == 0:
                base_copies[2].start()
                for later in range(len(cuts[1])):
                    load(1, *streams[1], later).start()
            elif tile == 1:
                for k in range(3):
                    load_all(k).start()
                for copy in firsts[3:]:
                    copy.start()
    with jax.named_scope("compute2"):
        base_copies[2].wait()
        for tile in range(len(cuts[1])):
            reduce_last(tile)
    stage_1()
    with jax.named_scope("project0"):
        project_pair()
        pl.semaphore_wait(near_sem, len(next_to))
        pl.semaphore_signal(
            across_sem, inc=1, device_id=(me, along_y(2)), device_id_type=MESH
        )
        for step in range(1, SIDE):
            pl.semaphore_signal(
                plane_sem, inc=1, device_id=(ahead(0, step), mt), device_id_type=MESH
            )
        send_parts(0)
        send_parts(1)
    with jax.named_scope("project2"):
        project_last()
        send_parts(2)
    stage_far(1)
    stage_on(0)
    with jax.named_scope("pass0"):
        pass_parts((0, 1))
    with jax.named_scope("pass2"):
        pass_parts((2,))
    stage_far(2)
    for copy in firsts[3:]:
        copy.wait()
    def total_copy(j):
        return pltpu.make_async_remote_copy(
            src_ref=totals.at[0],
            dst_ref=totals.at[j],
            send_sem=send_sem.at[6],
            recv_sem=sum_recv.at[1],
            device_id=(lax.rem(me + j, size), mt),
            device_id_type=MESH,
        )

    def sum_copy(j):
        return pltpu.make_async_remote_copy(
            src_ref=sums.at[0],
            dst_ref=sums.at[j],
            send_sem=send_sem.at[7],
            recv_sem=sum_recv.at[0],
            device_id=(me, lax.rem(mt + j, groups)),
            device_id_type=MESH,
        )

    def sums_arrived():
        return all_of(sums.at[pl.ds(1, groups - 1)], 7, sum_recv.at[0])

    def totals_arrived():
        return all_of(totals.at[pl.ds(1, size - 1)], 6, sum_recv.at[1])

    with jax.named_scope("combine0"):
        stage_on(1)
        own_sum = combine((0, 1))
    with jax.named_scope("combine2"):
        sums[0] = own_sum + combine((2,))
    pl.semaphore_wait(across_sem, 1)
    for j in range(1, groups):
        sum_copy(j).start()
    with jax.named_scope("stage2"):
        stage_3()
        stage_on(2)
    with jax.named_scope("dirs1"):
        pass_dirs((0, 1))
    with jax.named_scope("sums"):
        sums_arrived().wait_recv()
        total = sums[0]
        for j in range(1, groups):
            total = total + sums[j]
        totals[0] = total
        pl.semaphore_wait(plane_sem, SIDE - 1)
        for j in range(1, size):
            total_copy(j).start()

    with jax.named_scope("dirs1b"):
        pass_dirs((2,))
    with jax.named_scope("stage5"):
        stage_on(3)
    with jax.named_scope("dirs2"):
        all_of(got, 4, dir_recv.at[2]).wait_recv()
    with jax.named_scope("totals"):
        totals_arrived().wait_recv()
        for j in range(1, size):
            total = total + totals[j]
        scale = lax.rsqrt(total / entries + 1.0)
        for k in range(3):
            scale_ref[k] = jnp.broadcast_to(scale[:, k : k + 1], scale_ref.shape[1:])
    with jax.named_scope("stage6"):
        w_arrived(6)

    with jax.named_scope("drain"):
        all_of(all_w.at[pl.ds(0, size - 1)], 0, w_recv.at[0]).wait_send()
        all_of(got, 1, dir_recv.at[2]).wait_send()
        all_of(last, 2, dir_recv.at[0]).wait_send()
        all_of(last, 3, dir_recv.at[0]).wait_send()
        all_of(got, 4, dir_recv.at[2]).wait_send()
        pair_half(pl.ds(0, 3), pair_recv.at[0]).wait_send()
        totals_arrived().wait_send()
        sums_arrived().wait_send()


def exchange(size, groups, x, oc, fc, vc, go, bases, fw, vw, ow, m1, m2):
    tokens, width = x.shape
    rank = bases.shape[2]
    rows, columns = fw.shape
    rank_rows = m1.shape[1]
    bf16, f32 = jnp.bfloat16, jnp.float32
    vmem = pl.BlockSpec(memory_space=pltpu.VMEM)
    dma = pltpu.SemaphoreType.DMA
    kernel = functools.partial(
        exchange_kernel,
        size,
        groups,
        float(tokens * size) ** (-0.5),
        float(rank * columns * groups),
    )
    return pl.pallas_call(
        kernel,
        out_shape=(
            pltpu.VMEM((size, 3, rows, columns), bf16),
            pltpu.VMEM((3, SIDE, SIDE, rank_rows, columns), bf16),
            pltpu.VMEM(bases.shape, bf16),
            pltpu.VMEM((3, 8, 512), f32),
            pltpu.VMEM(m1.shape, f32),
            pltpu.VMEM(m2.shape, f32),
            pltpu.VMEM(fw.shape, f32),
            pltpu.VMEM(vw.shape, f32),
            pltpu.VMEM(ow.shape, f32),
        ),
        in_specs=[pl.BlockSpec(memory_space=pltpu.HBM)] * 11,
        out_specs=(vmem,) * 9,
        scratch_shapes=[
            pltpu.VMEM(m1.shape, f32),
            pltpu.VMEM(m2.shape, f32),
            pltpu.VMEM((tokens // 2, width), bf16),
            pltpu.VMEM((tokens // 2, width), bf16),
            pltpu.VMEM((3, tokens, columns), bf16),
            pltpu.VMEM((3, tokens, rank), bf16),
            pltpu.VMEM((3, SIDE, SIDE, rank_rows, columns), f32),
            pltpu.VMEM((3, SIDE, SIDE, rank_rows, columns), bf16),
            pltpu.VMEM((3, 2, SIDE - 1, SIDE, rank_rows, columns // 2), bf16),
            pltpu.VMEM((3, 2, SIDE, rank_rows, columns // 2), f32),
            pltpu.VMEM((3, 2, SIDE, rank_rows, columns // 2), bf16),
            pltpu.VMEM((3, 2, SIDE - 1, rank_rows, columns // 2), bf16),
            pltpu.VMEM((groups, 1, 128), f32),
            pltpu.VMEM((size, 1, 128), f32),
            dma((5,)),
            dma((2, 3)),
            dma((3,)),
            dma((3,)),
            dma((2,)),
            dma((8,)),
            dma((7,)),
            dma((2, 2)),
            dma((3,)),
            dma((2,)),
            pltpu.SemaphoreType.REGULAR,
            pltpu.SemaphoreType.REGULAR,
            pltpu.SemaphoreType.REGULAR,
        ],
        compiler_params=pltpu.CompilerParams(
            collective_id=0, has_side_effects=True, vmem_limit_bytes=52 * 1024 * 1024
        ),
    )(x, oc, fc, vc, go, bases, fw, vw, ow, m1, m2)


def finish_kernel(
    scale_ref,
    dirs_ref,
    all_w,
    bases_ref,
    fw_ref,
    vw_ref,
    ow_ref,
    n1_ref,
    n2_ref,
    new_f,
    new_v,
    new_o,
    copy_f,
    copy_v,
    copy_o,
    n1_out,
    n2_out,
    step_f,
    step_v,
    step_o,
    cf_buf,
    cv_buf,
    co_buf,
    down_buf,
    across_buf,
    tile_sem,
    small_sem,
):
    tiles = 4
    rows = cf_buf.shape[0] // tiles
    own = fw_ref.shape[0]
    owners = rows // own

    def put(src, dst, sem):
        pltpu.make_async_copy(src, dst, sem).start()

    put(n1_ref, n1_out, small_sem.at[0])
    put(n2_ref, n2_out, small_sem.at[1])

    def direction(k):
        return dirs_ref[k].reshape(bases_ref.shape[2], down_buf.shape[2])

    def down(at, k):
        step = jnp.dot(bases_ref[k, at, :], direction(k), preferred_element_type=jnp.float32)
        return step * scale_ref[k, 0:1, : step.shape[1]]

    def across(at):
        step = lax.dot_general(
            direction(2),
            bases_ref[2, at, :],
            (((0,), (1,)), ((), ())),
            preferred_element_type=jnp.float32,
        )
        return step * scale_ref[2, 0:1, : step.shape[1]]

    me = pl.ds(pl.multiple_of(lax.axis_index("fs") * own, own), own)
    for k, weight, new, out in ((0, fw_ref, new_f, step_f), (1, vw_ref, new_v, step_v)):
        step = down(me, k)
        down_buf[2 * k] = step
        put(down_buf.at[2 * k], out, small_sem.at[2])
        down_buf[2 * k + 1] = weight[...] - 0.01 * step
        put(down_buf.at[2 * k + 1], new, small_sem.at[2])
    step = across(me)
    across_buf[0] = step
    put(across_buf.at[0], step_o, small_sem.at[3])
    across_buf[1] = ow_ref[...] - 0.01 * step
    put(across_buf.at[1], new_o, small_sem.at[3])

    for tile in range(tiles):
        at = pl.ds(tile * rows, rows)
        owned = pl.ds(tile * owners, owners)
        for k, buf, out in ((0, cf_buf, copy_f), (1, cv_buf, copy_v)):
            old = all_w[owned, k].reshape(rows, cf_buf.shape[1])
            value = old.astype(jnp.float32) - 0.01 * down(at, k)
            buf[at, :] = value.astype(jnp.bfloat16)
            put(buf.at[at, :], out.at[at, :], tile_sem.at[k])
        step = across(at)
        for i in range(owners):
            lanes = pl.ds(tile * rows + i * own, own)
            for j in range(2):
                old = all_w[tile * owners + i, 2, :, j * own : (j + 1) * own]
                value = old.astype(jnp.float32) - 0.01 * step[
                    j * own : (j + 1) * own, i * own : (i + 1) * own
                ]
                co_buf[pl.ds(j * own, own), lanes] = value.astype(jnp.bfloat16)
        put(co_buf.at[:, at], copy_o.at[:, at], tile_sem.at[2])

    for i, buf, out in ((0, cf_buf, copy_f), (1, cv_buf, copy_v), (2, co_buf, copy_o)):
        pltpu.make_async_copy(buf, out, tile_sem.at[i]).wait()
    pltpu.make_async_copy(n1_ref, n1_out, small_sem.at[0]).wait()
    pltpu.make_async_copy(n2_ref, n2_out, small_sem.at[1]).wait()
    pltpu.make_async_copy(down_buf, down_buf, small_sem.at[2]).wait()
    pltpu.make_async_copy(across_buf, across_buf, small_sem.at[3]).wait()


def finish(all_w, dirs, bases, scales, one, two, fw, vw, ow):
    size, _, rows, columns = all_w.shape
    depth = size * rows
    rank = bases.shape[2]
    bf16, f32 = jnp.bfloat16, jnp.float32
    dma = pltpu.SemaphoreType.DMA
    tall = jax.ShapeDtypeStruct((depth, columns), bf16)
    wide = jax.ShapeDtypeStruct((columns, depth), bf16)
    down = jax.ShapeDtypeStruct((rows, columns), f32)
    across = jax.ShapeDtypeStruct((columns, rows), f32)
    small = jax.ShapeDtypeStruct(one.shape, f32)
    return pl.pallas_call(
        finish_kernel,
        out_shape=(down, down, across, tall, tall, wide, small, small, down, down, across),
        in_specs=[pl.BlockSpec(memory_space=pltpu.VMEM)] * 9,
        out_specs=(pl.BlockSpec(memory_space=pltpu.HBM),) * 11,
        scratch_shapes=[
            pltpu.VMEM(tall.shape, bf16),
            pltpu.VMEM(tall.shape, bf16),
            pltpu.VMEM(wide.shape, bf16),
            pltpu.VMEM((4,) + down.shape, f32),
            pltpu.VMEM((2,) + across.shape, f32),
            dma((3,)),
            dma((4,)),
        ],
        compiler_params=pltpu.CompilerParams(vmem_limit_bytes=24 * 1024 * 1024),
        cost_estimate=pl.CostEstimate(
            flops=6 * depth * rank * columns, bytes_accessed=8 * depth * columns, transcendentals=0
        ),
    )(scales, dirs, all_w, bases, fw, vw, ow, one, two)


def on_device(
    normed_input,
    forget_cot,
    value_cot,
    gated_output,
    output_cot,
    forget_weight,
    value_weight,
    out_weight,
    bases,
    first_moment,
    second_moment,
):
    size, groups = lax.axis_size("fs"), lax.axis_size("tp")
    held = exchange(
        size,
        groups,
        normed_input,
        output_cot,
        forget_cot,
        value_cot,
        gated_output,
        bases,
        forget_weight,
        value_weight,
        out_weight,
        first_moment.transpose(1, 0, 2),
        second_moment.transpose(1, 0, 2),
    )
    outs = finish(*held)
    return (
        *outs[:6],
        outs[6].transpose(1, 0, 2),
        outs[7].transpose(1, 0, 2),
        *outs[8:],
    )


def solution(mesh):
    placed = (
        P("fs", None),
        P("fs", "tp"),
        P("fs", "tp"),
        P("fs", "tp"),
        P("fs", None),
        P("fs", "tp"),
        P("fs", "tp"),
        P("tp", "fs"),
        P(),
        P("fs", None, "tp"),
        P("fs", None, "tp"),
    )
    return jax.shard_map(
        on_device,
        mesh=mesh,
        in_specs=placed,
        out_specs=(
            P("fs", "tp"),
            P("fs", "tp"),
            P("tp", "fs"),
            P(None, "tp"),
            P(None, "tp"),
            P("tp", None),
            P("fs", None, "tp"),
            P("fs", None, "tp"),
            P("fs", "tp"),
            P("fs", "tp"),
            P("tp", "fs"),
        ),
        check_vma=False,
    )
```

```python
import functools

import jax
import jax.numpy as jnp
from jax import lax
from jax.experimental import pallas as pl
from jax.experimental.pallas import tpu as pltpu
from jax.sharding import PartitionSpec as P

MESH = pl.DeviceIdType.MESH
SIDE = 4
STEPS = (1, -1)
OFFSETS = (0, -1, 1, 2)


def exchange_kernel(
    size,
    groups,
    factor,
    entries,
    x_hbm,
    oc_hbm,
    fc_hbm,
    vc_hbm,
    go_hbm,
    bases_hbm,
    fw_hbm,
    vw_hbm,
    ow_hbm,
    m1_hbm,
    m2_hbm,
    all_w,
    dirs,
    b_buf,
    scale_ref,
    n1_ref,
    n2_ref,
    fw_ref,
    vw_ref,
    ow_ref,
    m1_ref,
    m2_ref,
    x_buf,
    oc_buf,
    c_buf,
    red,
    acc,
    part,
    got,
    held,
    mid,
    last,
    sums,
    totals,
    first_sem,
    load_sem,
    cot_sem,
    base_sem,
    pair_recv,
    send_sem,
    w_recv,
    part_recv,
    dir_recv,
    sum_recv,
    near_sem,
    across_sem,
):
    me = lax.axis_index("fs")
    mt = lax.axis_index("tp")
    z = lax.div(me, SIDE)
    x = lax.rem(me, SIDE)
    core = lax.rem(mt, 2)
    partner = mt + 1 - 2 * core
    tokens = c_buf.shape[1]
    quarter_rows = x_buf.shape[0] // 4
    cuts = (((0, 1), (1, 2), (3, 1)), ((0, 2), (2, 2)))
    first_row = core * x_buf.shape[0]
    rank_rows = m1_ref.shape[1]
    columns = m1_ref.shape[2]
    own = fw_ref.shape[0]
    half_rows = own // 2

    firsts = [
        pltpu.make_async_copy(src, dst, first_sem.at[i])
        for i, (src, dst) in enumerate(
            (
                (fw_hbm, fw_ref),
                (vw_hbm, vw_ref),
                (ow_hbm, ow_ref),
                (m1_hbm, m1_ref),
                (m2_hbm, m2_ref),
            )
        )
    ]
    for copy in firsts[:3]:
        copy.start()
    base_copies = [
        pltpu.make_async_copy(bases_hbm.at[k], b_buf.at[k], base_sem.at[k]) for k in range(3)
    ]

    def tile_rows(which, tile):
        start, count = cuts[which][tile]
        rows = count * quarter_rows
        return pl.ds(pl.multiple_of(first_row + start * quarter_rows, quarter_rows), rows)

    def held_rows(which, tile):
        start, count = cuts[which][tile]
        return pl.ds(start * quarter_rows, count * quarter_rows)

    def load(which, src, dst, tile):
        return pltpu.make_async_copy(
            src.at[tile_rows(which, tile), :],
            dst.at[held_rows(which, tile), :],
            load_sem.at[which, tile],
        )

    def load_all(k):
        return pltpu.make_async_copy((fc_hbm, vc_hbm, go_hbm)[k], c_buf.at[k], cot_sem.at[k])

    streams = ((x_hbm, x_buf), (oc_hbm, oc_buf))
    base_copies[0].start()
    load(0, *streams[0], 0).start()
    base_copies[1].start()

    def ahead(dz, dx):
        return lax.rem(z + dz, SIDE) * SIDE + lax.rem(x + dx, SIDE)

    def along_y(step):
        return lax.rem(mt + 2 * step, groups)

    barrier = pltpu.get_barrier_semaphore()
    around = [(ahead(0, 1), mt), (ahead(0, 3), mt), (ahead(1, 0), mt), (ahead(3, 0), mt)]
    around += [(me, along_y(1)), (me, along_y(3)), (me, partner)]
    for place in around:
        pl.semaphore_signal(barrier, inc=1, device_id=place, device_id_type=MESH)
    for copy in firsts[:3]:
        copy.wait()
    all_w[me, 0] = fw_ref[...].astype(jnp.bfloat16)
    all_w[me, 1] = vw_ref[...].astype(jnp.bfloat16)
    all_w[me, 2, :, :own] = ow_ref[:own, :].astype(jnp.bfloat16)
    all_w[me, 2, :, own:] = ow_ref[own:, :].astype(jnp.bfloat16)

    def node(h, a, b):
        dz, dx = (b, a) if h == 0 else (a, b)
        return lax.rem(z + dz + SIDE, SIDE) * SIDE + lax.rem(x + dx + SIDE, SIDE)

    def w_copy(h, slot, owner, quarter, dest):
        start, count = h * half_rows, half_rows
        if quarter is not None:
            count = half_rows // 2
            start = start + quarter * count
        view = all_w.at[owner, :, pl.ds(start, count), :]
        return pltpu.make_async_remote_copy(
            src_ref=view,
            dst_ref=view,
            send_sem=send_sem.at[0],
            recv_sem=w_recv.at[slot],
            device_id=(dest, mt),
            device_id_type=MESH,
        )

    def near(h, s):
        return w_copy(h, 0, me, None, node(h, STEPS[s], 0))

    def near_on(h, s):
        return w_copy(h, 1, node(h, -STEPS[s], 0), s, node(h, STEPS[s], 0))

    def far(h, i, s):
        return w_copy(h, 2 + i, node(h, OFFSETS[i], 0), None, node(h, 0, STEPS[s]))

    def far_on(h, i, s):
        return w_copy(h, 6, node(h, OFFSETS[i], -STEPS[s]), s, node(h, 0, STEPS[s]))

    def all_of(view, send, recv, to=None):
        return pltpu.make_async_remote_copy(
            src_ref=view,
            dst_ref=view,
            send_sem=send_sem.at[send],
            recv_sem=recv,
            device_id=(node(0, 1, 0), mt) if to is None else to,
            device_id_type=MESH,
        )

    def w_arrived(slot):
        count = (2, 1, 2, 2, 2, 2, 4)[slot]
        all_of(all_w.at[pl.ds(0, count)], 0, w_recv.at[slot]).wait_recv()

    def each(start):
        for h in range(2):
            for s in range(2):
                start(h, s).start()

    def stage_0():
        each(near)
        stage_far(0)

    def stage_1():
        w_arrived(0)
        each(near_on)

    def stage_far(i):
        each(lambda h, s: far(h, i, s))

    def stage_on(i):
        w_arrived(2 + i)
        each(lambda h, s: far_on(h, i, s))

    def stage_3():
        w_arrived(1)
        stage_far(3)

    half_cols = columns // 2

    def cut(h):
        return pl.ds(h * half_cols, half_cols)

    def line(h, second, j):
        first_axis = (h == 0) != second
        return (
            z * SIDE + lax.rem(x + j, SIDE) if first_axis else lax.rem(z + j, SIDE) * SIDE + x
        )

    def blocks(ref, k, h, j):
        if h == 0:
            return ref.at[k, :, lax.rem(x + j, SIDE), :, cut(h)]
        return ref.at[k, lax.rem(z + j, SIDE), :, :, cut(h)]

    def move(src, dst, send, recv, dest):
        return pltpu.make_async_remote_copy(
            src_ref=src,
            dst_ref=dst,
            send_sem=send_sem.at[send],
            recv_sem=recv,
            device_id=(dest, mt),
            device_id_type=MESH,
        )

    def part_first(k, h, j):
        return move(
            blocks(part, k, h, j), got.at[k, h, j - 1], 1, part_recv.at[0, k // 2], line(h, False, j)
        )

    def part_second(k, h, j):
        place = lax.rem((z if h == 0 else x) + j, SIDE)
        return move(
            mid.at[k, h, place], last.at[k, h, j - 1], 2, part_recv.at[1, k // 2], line(h, True, j)
        )

    def dir_first(k, h, j):
        view = dirs.at[k, z, x, :, cut(h)]
        return move(view, view, 3, dir_recv.at[k // 2], line(h, False, j))

    def dir_second(k, h, j):
        view = dirs.at[k, z, :, :, cut(h)] if h == 0 else dirs.at[k, :, x, :, cut(h)]
        return move(view, view, 4, dir_recv.at[2], line(h, True, j))

    def group_of(ref, ks):
        return ref.at[pl.ds(ks[0], len(ks))]

    ALL = [(h, j) for h in range(2) for j in range(1, SIDE)]

    def send_parts(k):
        for h, j in ALL:
            part_first(k, h, j).start()

    def pass_parts(ks):
        all_of(group_of(got, ks), 1, part_recv.at[0, ks[0] // 2]).wait_recv()
        for k in ks:
            for h in range(2):
                own_part = acc[k, :, x, :, cut(h)] if h == 0 else acc[k, z, :, :, cut(h)]
                total = own_part * factor
                for j in range(1, SIDE):
                    total = total + got[k, h, j - 1].astype(jnp.float32)
                held[k, h] = total
                mid[k, h] = total.astype(jnp.bfloat16)
                for j in range(1, SIDE):
                    part_second(k, h, j).start()

    lane = lax.broadcasted_iota(jnp.int32, sums.shape[1:], 1)

    def combine(ks):
        all_of(group_of(last, ks), 2, part_recv.at[1, ks[0] // 2]).wait_recv()
        return sum(update(k) for k in ks)

    def update(k):
        square = jnp.zeros((rank_rows, half_cols), jnp.float32)
        for h in range(2):
            projected = held[k, h, z if h == 0 else x]
            for j in range(1, SIDE):
                projected = projected + last[k, h, j - 1].astype(jnp.float32)
            one = 0.9 * m1_ref[k, :, cut(h)] + 0.1 * projected
            two = 0.9 * m2_ref[k, :, cut(h)] + 0.1 * projected * projected
            n1_ref[k, :, cut(h)] = one
            n2_ref[k, :, cut(h)] = two
            rounded = (one / (jnp.sqrt(two) + 1e-08)).astype(jnp.bfloat16)
            dirs[k, z, x, :, cut(h)] = rounded
            for j in range(1, SIDE):
                dir_first(k, h, j).start()
            value = rounded.astype(jnp.float32)
            square = square + value * value
        return jnp.where(lane == k, jnp.sum(square), 0.0)

    def pass_dirs(ks):
        all_of(group_of(last, ks), 3, dir_recv.at[ks[0] // 2]).wait_recv()
        for k in ks:
            for h, j in ALL:
                dir_second(k, h, j).start()

    def pair_copy(k, tile):
        view = red.at[k, tile_rows(k // 2, tile), :]
        return pltpu.make_async_remote_copy(
            src_ref=view,
            dst_ref=view,
            send_sem=send_sem.at[5],
            recv_sem=pair_recv.at[k // 2],
            device_id=(me, partner),
            device_id_type=MESH,
        )

    def pair_half(ks, recv):
        view = red.at[ks, pl.ds(0, tokens // 2), :]
        return all_of(view, 5, recv, (me, partner))

    def reduce_pair(tile):
        load(0, *streams[0], tile).wait()
        rows = x_buf[held_rows(0, tile), :]
        at = tile_rows(0, tile)
        first = jnp.dot(rows, b_buf[0], preferred_element_type=jnp.float32)
        second = jnp.dot(rows, b_buf[1], preferred_element_type=jnp.float32)
        red[0, at, :] = first.astype(jnp.bfloat16)
        red[1, at, :] = second.astype(jnp.bfloat16)
        for k in range(2):
            pair_copy(k, tile).start()

    def reduce_last(tile):
        load(1, *streams[1], tile).wait()
        start, count = cuts[1][tile]
        half = count * quarter_rows // 2
        upper = pl.ds(start * quarter_rows, half)
        lower = pl.ds(start * quarter_rows + half, half)
        first = jnp.dot(oc_buf[upper, :], b_buf[2], preferred_element_type=jnp.float32)
        second = jnp.dot(oc_buf[lower, :], b_buf[2], preferred_element_type=jnp.float32)
        both = jnp.concatenate([first, second], axis=0)
        red[2, tile_rows(1, tile), :] = both.astype(jnp.bfloat16)
        pair_copy(2, tile).start()

    def fold(left, right):
        return lax.dot_general(
            left, right, (((0,), (0,)), ((), ())), preferred_element_type=jnp.float32
        )

    def project_pair():
        for k in range(2):
            load_all(k).wait()
        pair_half(pl.ds(0, 2), pair_recv.at[0]).wait_recv()
        shape = acc.shape[1:]
        first = fold(red[0], c_buf[0])
        second = fold(red[1], c_buf[1])
        acc[0] = first.reshape(shape)
        acc[1] = second.reshape(shape)
        part[0] = (first * factor).astype(jnp.bfloat16).reshape(shape)
        part[1] = (second * factor).astype(jnp.bfloat16).reshape(shape)

    def project_last():
        load_all(2).wait()
        pair_half(pl.ds(2, 1), pair_recv.at[1]).wait_recv()
        half = tokens // 2
        total = fold(red[2, :half, :], c_buf[2, :half, :])
        total = total + fold(red[2, half:, :], c_buf[2, half:, :])
        acc[2] = total.reshape(acc.shape[1:])
        part[2] = (total * factor).astype(jnp.bfloat16).reshape(acc.shape[1:])

    for tile in range(1, len(cuts[0])):
        load(0, *streams[0], tile).start()
    with jax.named_scope("barrier"):
        pl.semaphore_wait(barrier, len(around))
    next_to = [around[0], around[2], around[4], around[5]]
    for place in next_to:
        pl.semaphore_signal(near_sem, inc=1, device_id=place, device_id_type=MESH)
    stage_0()
    with jax.named_scope("compute0"):
        for k in range(2):
            base_copies[k].wait()
        for tile in range(len(cuts[0])):
            reduce_pair(tile)
            if tile == 0:
                base_copies[2].start()
                for later in range(len(cuts[1])):
                    load(1, *streams[1], later).start()
            elif tile == 1:
                for k in range(3):
                    load_all(k).start()
                for copy in firsts[3:]:
                    copy.start()
    with jax.named_scope("compute2"):
        base_copies[2].wait()
        for tile in range(len(cuts[1])):
            reduce_last(tile)
    stage_1()
    with jax.named_scope("project0"):
        project_pair()
        pl.semaphore_wait(near_sem, len(next_to))
        pl.semaphore_signal(
            across_sem, inc=1, device_id=(me, along_y(2)), device_id_type=MESH
        )
        send_parts(0)
        send_parts(1)
    with jax.named_scope("project2"):
        project_last()
        send_parts(2)
    stage_far(1)
    stage_on(0)
    with jax.named_scope("pass0"):
        pl.semaphore_wait(across_sem, 1)
        pass_parts((0, 1))
    with jax.named_scope("pass2"):
        pass_parts((2,))
    stage_far(2)
    for copy in firsts[3:]:
        copy.wait()
    def total_copy(j):
        return pltpu.make_async_remote_copy(
            src_ref=totals.at[0],
            dst_ref=totals.at[j],
            send_sem=send_sem.at[6],
            recv_sem=sum_recv.at[1],
            device_id=(ahead(0, j), mt),
            device_id_type=MESH,
        )

    def sum_copy(j):
        return pltpu.make_async_remote_copy(
            src_ref=sums.at[0],
            dst_ref=sums.at[j],
            send_sem=send_sem.at[7],
            recv_sem=sum_recv.at[0],
            device_id=(ahead(j // groups, 0), lax.rem(mt + j % groups, groups)),
            device_id_type=MESH,
        )

    def sums_arrived():
        return all_of(sums.at[pl.ds(1, SIDE * groups - 1)], 7, sum_recv.at[0])

    def totals_arrived():
        return all_of(totals.at[pl.ds(1, SIDE - 1)], 6, sum_recv.at[1])

    with jax.named_scope("combine0"):
        stage_on(1)
        own_sum = combine((0, 1))
    with jax.named_scope("combine2"):
        sums[0] = own_sum + combine((2,))
    for j in range(1, SIDE * groups):
        sum_copy(j).start()
    with jax.named_scope("stage2"):
        stage_3()
        stage_on(2)
    with jax.named_scope("dirs1"):
        pass_dirs((0, 1))
    with jax.named_scope("dirs1b"):
        pass_dirs((2,))
    with jax.named_scope("stage5n"):
        pl.when(core == 1)(lambda: stage_on(3))
    with jax.named_scope("sums"):
        sums_arrived().wait_recv()
        total = sums[0]
        for j in range(1, SIDE * groups):
            total = total + sums[j]
        totals[0] = total
        for j in range(1, SIDE):
            total_copy(j).start()

    with jax.named_scope("stage5"):
        pl.when(core == 0)(lambda: stage_on(3))
    with jax.named_scope("dirs2"):
        all_of(got, 4, dir_recv.at[2]).wait_recv()
    with jax.named_scope("totals"):
        totals_arrived().wait_recv()
        for j in range(1, SIDE):
            total = total + totals[j]
        scale = lax.rsqrt(total / entries + 1.0)
        for k in range(3):
            scale_ref[k] = jnp.broadcast_to(scale[:, k : k + 1], scale_ref.shape[1:])
    with jax.named_scope("stage6"):
        w_arrived(6)

    with jax.named_scope("drain"):
        all_of(all_w.at[pl.ds(0, size - 1)], 0, w_recv.at[0]).wait_send()
        all_of(got, 1, dir_recv.at[2]).wait_send()
        all_of(last, 2, dir_recv.at[0]).wait_send()
        all_of(last, 3, dir_recv.at[0]).wait_send()
        all_of(got, 4, dir_recv.at[2]).wait_send()
        pair_half(pl.ds(0, 3), pair_recv.at[0]).wait_send()
        totals_arrived().wait_send()
        sums_arrived().wait_send()


def exchange(size, groups, x, oc, fc, vc, go, bases, fw, vw, ow, m1, m2):
    tokens, width = x.shape
    rank = bases.shape[2]
    rows, columns = fw.shape
    rank_rows = m1.shape[1]
    bf16, f32 = jnp.bfloat16, jnp.float32
    vmem = pl.BlockSpec(memory_space=pltpu.VMEM)
    dma = pltpu.SemaphoreType.DMA
    kernel = functools.partial(
        exchange_kernel,
        size,
        groups,
        float(tokens * size) ** (-0.5),
        float(rank * columns * groups),
    )
    return pl.pallas_call(
        kernel,
        out_shape=(
            pltpu.VMEM((size, 3, rows, columns), bf16),
            pltpu.VMEM((3, SIDE, SIDE, rank_rows, columns), bf16),
            pltpu.VMEM(bases.shape, bf16),
            pltpu.VMEM((3, 8, 512), f32),
            pltpu.VMEM(m1.shape, f32),
            pltpu.VMEM(m2.shape, f32),
            pltpu.VMEM(fw.shape, f32),
            pltpu.VMEM(vw.shape, f32),
            pltpu.VMEM(ow.shape, f32),
        ),
        in_specs=[pl.BlockSpec(memory_space=pltpu.HBM)] * 11,
        out_specs=(vmem,) * 9,
        scratch_shapes=[
            pltpu.VMEM(m1.shape, f32),
            pltpu.VMEM(m2.shape, f32),
            pltpu.VMEM((tokens // 2, width), bf16),
            pltpu.VMEM((tokens // 2, width), bf16),
            pltpu.VMEM((3, tokens, columns), bf16),
            pltpu.VMEM((3, tokens, rank), bf16),
            pltpu.VMEM((3, SIDE, SIDE, rank_rows, columns), f32),
            pltpu.VMEM((3, SIDE, SIDE, rank_rows, columns), bf16),
            pltpu.VMEM((3, 2, SIDE - 1, SIDE, rank_rows, columns // 2), bf16),
            pltpu.VMEM((3, 2, SIDE, rank_rows, columns // 2), f32),
            pltpu.VMEM((3, 2, SIDE, rank_rows, columns // 2), bf16),
            pltpu.VMEM((3, 2, SIDE - 1, rank_rows, columns // 2), bf16),
            pltpu.VMEM((SIDE * groups, 1, 128), f32),
            pltpu.VMEM((SIDE, 1, 128), f32),
            dma((5,)),
            dma((2, 3)),
            dma((3,)),
            dma((3,)),
            dma((2,)),
            dma((8,)),
            dma((7,)),
            dma((2, 2)),
            dma((3,)),
            dma((2,)),
            pltpu.SemaphoreType.REGULAR,
            pltpu.SemaphoreType.REGULAR,
        ],
        compiler_params=pltpu.CompilerParams(
            collective_id=0, has_side_effects=True, vmem_limit_bytes=52 * 1024 * 1024
        ),
    )(x, oc, fc, vc, go, bases, fw, vw, ow, m1, m2)


def finish_kernel(
    scale_ref,
    dirs_ref,
    all_w,
    bases_ref,
    fw_ref,
    vw_ref,
    ow_ref,
    n1_ref,
    n2_ref,
    new_f,
    new_v,
    new_o,
    copy_f,
    copy_v,
    copy_o,
    n1_out,
    n2_out,
    step_f,
    step_v,
    step_o,
    cf_buf,
    cv_buf,
    co_buf,
    down_buf,
    across_buf,
    tile_sem,
    small_sem,
):
    tiles = 4
    rows = cf_buf.shape[0] // tiles
    own = fw_ref.shape[0]
    owners = rows // own

    def put(src, dst, sem):
        pltpu.make_async_copy(src, dst, sem).start()

    put(n1_ref, n1_out, small_sem.at[0])
    put(n2_ref, n2_out, small_sem.at[1])

    def direction(k):
        return dirs_ref[k].reshape(bases_ref.shape[2], down_buf.shape[2])

    def down(at, k):
        step = jnp.dot(bases_ref[k, at, :], direction(k), preferred_element_type=jnp.float32)
        return step * scale_ref[k, 0:1, : step.shape[1]]

    def across(at):
        step = lax.dot_general(
            direction(2),
            bases_ref[2, at, :],
            (((0,), (1,)), ((), ())),
            preferred_element_type=jnp.float32,
        )
        return step * scale_ref[2, 0:1, : step.shape[1]]

    me = pl.ds(pl.multiple_of(lax.axis_index("fs") * own, own), own)
    for k, weight, new, out in ((0, fw_ref, new_f, step_f), (1, vw_ref, new_v, step_v)):
        step = down(me, k)
        down_buf[2 * k] = step
        put(down_buf.at[2 * k], out, small_sem.at[2])
        down_buf[2 * k + 1] = weight[...] - 0.01 * step
        put(down_buf.at[2 * k + 1], new, small_sem.at[2])
    step = across(me)
    across_buf[0] = step
    put(across_buf.at[0], step_o, small_sem.at[3])
    across_buf[1] = ow_ref[...] - 0.01 * step
    put(across_buf.at[1], new_o, small_sem.at[3])

    for tile in range(tiles):
        at = pl.ds(tile * rows, rows)
        owned = pl.ds(tile * owners, owners)
        for k, buf, out in ((0, cf_buf, copy_f), (1, cv_buf, copy_v)):
            old = all_w[owned, k].reshape(rows, cf_buf.shape[1])
            value = old.astype(jnp.float32) - 0.01 * down(at, k)
            buf[at, :] = value.astype(jnp.bfloat16)
            put(buf.at[at, :], out.at[at, :], tile_sem.at[k])
        step = across(at)
        for i in range(owners):
            lanes = pl.ds(tile * rows + i * own, own)
            for j in range(2):
                old = all_w[tile * owners + i, 2, :, j * own : (j + 1) * own]
                value = old.astype(jnp.float32) - 0.01 * step[
                    j * own : (j + 1) * own, i * own : (i + 1) * own
                ]
                co_buf[pl.ds(j * own, own), lanes] = value.astype(jnp.bfloat16)
        put(co_buf.at[:, at], copy_o.at[:, at], tile_sem.at[2])

    for i, buf, out in ((0, cf_buf, copy_f), (1, cv_buf, copy_v), (2, co_buf, copy_o)):
        pltpu.make_async_copy(buf, out, tile_sem.at[i]).wait()
    pltpu.make_async_copy(n1_ref, n1_out, small_sem.at[0]).wait()
    pltpu.make_async_copy(n2_ref, n2_out, small_sem.at[1]).wait()
    pltpu.make_async_copy(down_buf, down_buf, small_sem.at[2]).wait()
    pltpu.make_async_copy(across_buf, across_buf, small_sem.at[3]).wait()


def finish(all_w, dirs, bases, scales, one, two, fw, vw, ow):
    size, _, rows, columns = all_w.shape
    depth = size * rows
    rank = bases.shape[2]
    bf16, f32 = jnp.bfloat16, jnp.float32
    dma = pltpu.SemaphoreType.DMA
    tall = jax.ShapeDtypeStruct((depth, columns), bf16)
    wide = jax.ShapeDtypeStruct((columns, depth), bf16)
    down = jax.ShapeDtypeStruct((rows, columns), f32)
    across = jax.ShapeDtypeStruct((columns, rows), f32)
    small = jax.ShapeDtypeStruct(one.shape, f32)
    return pl.pallas_call(
        finish_kernel,
        out_shape=(down, down, across, tall, tall, wide, small, small, down, down, across),
        in_specs=[pl.BlockSpec(memory_space=pltpu.VMEM)] * 9,
        out_specs=(pl.BlockSpec(memory_space=pltpu.HBM),) * 11,
        scratch_shapes=[
            pltpu.VMEM(tall.shape, bf16),
            pltpu.VMEM(tall.shape, bf16),
            pltpu.VMEM(wide.shape, bf16),
            pltpu.VMEM((4,) + down.shape, f32),
            pltpu.VMEM((2,) + across.shape, f32),
            dma((3,)),
            dma((4,)),
        ],
        compiler_params=pltpu.CompilerParams(vmem_limit_bytes=24 * 1024 * 1024),
        cost_estimate=pl.CostEstimate(
            flops=6 * depth * rank * columns, bytes_accessed=8 * depth * columns, transcendentals=0
        ),
    )(scales, dirs, all_w, bases, fw, vw, ow, one, two)


def on_device(
    normed_input,
    forget_cot,
    value_cot,
    gated_output,
    output_cot,
    forget_weight,
    value_weight,
    out_weight,
    bases,
    first_moment,
    second_moment,
):
    size, groups = lax.axis_size("fs"), lax.axis_size("tp")
    held = exchange(
        size,
        groups,
        normed_input,
        output_cot,
        forget_cot,
        value_cot,
        gated_output,
        bases,
        forget_weight,
        value_weight,
        out_weight,
        first_moment.transpose(1, 0, 2),
        second_moment.transpose(1, 0, 2),
    )
    outs = finish(*held)
    return (
        *outs[:6],
        outs[6].transpose(1, 0, 2),
        outs[7].transpose(1, 0, 2),
        *outs[8:],
    )


def solution(mesh):
    placed = (
        P("fs", None),
        P("fs", "tp"),
        P("fs", "tp"),
        P("fs", "tp"),
        P("fs", None),
        P("fs", "tp"),
        P("fs", "tp"),
        P("tp", "fs"),
        P(),
        P("fs", None, "tp"),
        P("fs", None, "tp"),
    )
    return jax.shard_map(
        on_device,
        mesh=mesh,
        in_specs=placed,
        out_specs=(
            P("fs", "tp"),
            P("fs", "tp"),
            P("tp", "fs"),
            P(None, "tp"),
            P(None, "tp"),
            P("tp", None),
            P("fs", None, "tp"),
            P("fs", None, "tp"),
            P("fs", "tp"),
            P("fs", "tp"),
            P("tp", "fs"),
        ),
        check_vma=False,
    )
```

```python
import functools

import jax
import jax.numpy as jnp
from jax import lax
from jax.experimental import pallas as pl
from jax.experimental.pallas import tpu as pltpu
from jax.sharding import PartitionSpec as P

MESH = pl.DeviceIdType.MESH
SIDE = 4
STEPS = (1, -1)
OFFSETS = (0, -1, 1, 2)


def exchange_kernel(
    size,
    groups,
    factor,
    entries,
    x_hbm,
    oc_hbm,
    fc_hbm,
    vc_hbm,
    go_hbm,
    bases_hbm,
    fw_hbm,
    vw_hbm,
    ow_hbm,
    m1_hbm,
    m2_hbm,
    all_w,
    dirs,
    b_buf,
    scale_ref,
    n1_ref,
    n2_ref,
    fw_ref,
    vw_ref,
    ow_ref,
    m1_ref,
    m2_ref,
    x_buf,
    oc_buf,
    c_buf,
    red,
    acc,
    part,
    got,
    held,
    mid,
    last,
    sums,
    totals,
    first_sem,
    load_sem,
    cot_sem,
    base_sem,
    pair_recv,
    send_sem,
    w_recv,
    part_recv,
    dir_recv,
    sum_recv,
    near_sem,
    across_sem,
):
    me = lax.axis_index("fs")
    mt = lax.axis_index("tp")
    z = lax.div(me, SIDE)
    x = lax.rem(me, SIDE)
    core = lax.rem(mt, 2)
    partner = mt + 1 - 2 * core
    tokens = c_buf.shape[1]
    quarter_rows = x_buf.shape[0] // 4
    cuts = (((0, 1), (1, 2), (3, 1)), ((0, 2), (2, 2)))
    first_row = core * x_buf.shape[0]
    rank_rows = m1_ref.shape[1]
    columns = m1_ref.shape[2]
    own = fw_ref.shape[0]
    half_rows = own // 2

    firsts = [
        pltpu.make_async_copy(src, dst, first_sem.at[i])
        for i, (src, dst) in enumerate(
            (
                (fw_hbm, fw_ref),
                (vw_hbm, vw_ref),
                (ow_hbm, ow_ref),
                (m1_hbm, m1_ref),
                (m2_hbm, m2_ref),
            )
        )
    ]
    for copy in firsts[:3]:
        copy.start()
    base_copies = [
        pltpu.make_async_copy(bases_hbm.at[k], b_buf.at[k], base_sem.at[k]) for k in range(3)
    ]

    def tile_rows(which, tile):
        start, count = cuts[which][tile]
        rows = count * quarter_rows
        return pl.ds(pl.multiple_of(first_row + start * quarter_rows, quarter_rows), rows)

    def held_rows(which, tile):
        start, count = cuts[which][tile]
        return pl.ds(start * quarter_rows, count * quarter_rows)

    def load(which, src, dst, tile):
        return pltpu.make_async_copy(
            src.at[tile_rows(which, tile), :],
            dst.at[held_rows(which, tile), :],
            load_sem.at[which, tile],
        )

    def load_all(k):
        return pltpu.make_async_copy((fc_hbm, vc_hbm, go_hbm)[k], c_buf.at[k], cot_sem.at[k])

    streams = ((x_hbm, x_buf), (oc_hbm, oc_buf))
    base_copies[0].start(priority=1)
    load(0, *streams[0], 0).start(priority=1)
    base_copies[1].start(priority=1)

    def ahead(dz, dx):
        return lax.rem(z + dz, SIDE) * SIDE + lax.rem(x + dx, SIDE)

    def along_y(step):
        return lax.rem(mt + 2 * step, groups)

    barrier = pltpu.get_barrier_semaphore()
    around = [(ahead(0, 1), mt), (ahead(0, 3), mt), (ahead(1, 0), mt), (ahead(3, 0), mt)]
    around += [(me, along_y(1)), (me, along_y(3)), (me, partner)]
    for place in around:
        pl.semaphore_signal(barrier, inc=1, device_id=place, device_id_type=MESH)
    for copy in firsts[:3]:
        copy.wait()
    all_w[me, 0] = fw_ref[...].astype(jnp.bfloat16)
    all_w[me, 1] = vw_ref[...].astype(jnp.bfloat16)
    all_w[me, 2, :, :own] = ow_ref[:own, :].astype(jnp.bfloat16)
    all_w[me, 2, :, own:] = ow_ref[own:, :].astype(jnp.bfloat16)

    def node(h, a, b):
        dz, dx = (b, a) if h == 0 else (a, b)
        return lax.rem(z + dz + SIDE, SIDE) * SIDE + lax.rem(x + dx + SIDE, SIDE)

    def w_copy(h, slot, owner, quarter, dest):
        start, count = h * half_rows, half_rows
        if quarter is not None:
            count = half_rows // 2
            start = start + quarter * count
        view = all_w.at[owner, :, pl.ds(start, count), :]
        return pltpu.make_async_remote_copy(
            src_ref=view,
            dst_ref=view,
            send_sem=send_sem.at[0],
            recv_sem=w_recv.at[slot],
            device_id=(dest, mt),
            device_id_type=MESH,
        )

    def near(h, s):
        return w_copy(h, 0, me, None, node(h, STEPS[s], 0))

    def near_on(h, s):
        return w_copy(h, 1, node(h, -STEPS[s], 0), s, node(h, STEPS[s], 0))

    def far(h, i, s):
        return w_copy(h, 2 + i, node(h, OFFSETS[i], 0), None, node(h, 0, STEPS[s]))

    def far_on(h, i, s):
        return w_copy(h, 6, node(h, OFFSETS[i], -STEPS[s]), s, node(h, 0, STEPS[s]))

    def all_of(view, send, recv, to=None):
        return pltpu.make_async_remote_copy(
            src_ref=view,
            dst_ref=view,
            send_sem=send_sem.at[send],
            recv_sem=recv,
            device_id=(node(0, 1, 0), mt) if to is None else to,
            device_id_type=MESH,
        )

    def w_arrived(slot):
        count = (2, 1, 2, 2, 2, 2, 4)[slot]
        all_of(all_w.at[pl.ds(0, count)], 0, w_recv.at[slot]).wait_recv()

    def each(start):
        for h in range(2):
            for s in range(2):
                start(h, s).start()

    def stage_0():
        each(near)
        stage_far(0)

    def stage_1():
        w_arrived(0)
        each(near_on)

    def stage_far(i):
        each(lambda h, s: far(h, i, s))

    def stage_on(i):
        w_arrived(2 + i)
        each(lambda h, s: far_on(h, i, s))

    def stage_3():
        w_arrived(1)
        stage_far(3)

    half_cols = columns // 2

    def cut(h):
        return pl.ds(h * half_cols, half_cols)

    def line(h, second, j):
        first_axis = (h == 0) != second
        return (
            z * SIDE + lax.rem(x + j, SIDE) if first_axis else lax.rem(z + j, SIDE) * SIDE + x
        )

    def blocks(ref, k, h, j):
        if h == 0:
            return ref.at[k, :, lax.rem(x + j, SIDE), :, cut(h)]
        return ref.at[k, lax.rem(z + j, SIDE), :, :, cut(h)]

    def move(src, dst, send, recv, dest):
        return pltpu.make_async_remote_copy(
            src_ref=src,
            dst_ref=dst,
            send_sem=send_sem.at[send],
            recv_sem=recv,
            device_id=(dest, mt),
            device_id_type=MESH,
        )

    def part_first(k, h, j):
        return move(
            blocks(part, k, h, j), got.at[k, h, j - 1], 1, part_recv.at[0, k // 2], line(h, False, j)
        )

    def part_second(k, h, j):
        place = lax.rem((z if h == 0 else x) + j, SIDE)
        return move(
            mid.at[k, h, place], last.at[k, h, j - 1], 2, part_recv.at[1, k // 2], line(h, True, j)
        )

    def dir_first(k, h, j):
        view = dirs.at[k, z, x, :, cut(h)]
        return move(view, view, 3, dir_recv.at[k // 2], line(h, False, j))

    def dir_second(k, h, j):
        view = dirs.at[k, z, :, :, cut(h)] if h == 0 else dirs.at[k, :, x, :, cut(h)]
        return move(view, view, 4, dir_recv.at[2], line(h, True, j))

    def group_of(ref, ks):
        return ref.at[pl.ds(ks[0], len(ks))]

    FIRST = (2, 1, 3)
    ALL = [(h, j) for j in FIRST for h in range(2)]

    def send_parts(k):
        for h, j in ALL:
            part_first(k, h, j).start()

    def pass_parts(ks):
        all_of(group_of(got, ks), 1, part_recv.at[0, ks[0] // 2]).wait_recv()
        for k in ks:
            for h in range(2):
                own_part = acc[k, :, x, :, cut(h)] if h == 0 else acc[k, z, :, :, cut(h)]
                total = own_part * factor
                for j in range(1, SIDE):
                    total = total + got[k, h, j - 1].astype(jnp.float32)
                held[k, h] = total
                mid[k, h] = total.astype(jnp.bfloat16)
                for j in FIRST:
                    part_second(k, h, j).start()

    lane = lax.broadcasted_iota(jnp.int32, sums.shape[1:], 1)

    def combine(ks):
        all_of(group_of(last, ks), 2, part_recv.at[1, ks[0] // 2]).wait_recv()
        return sum(update(k) for k in ks)

    def update(k):
        square = jnp.zeros((rank_rows, half_cols), jnp.float32)
        for h in range(2):
            projected = held[k, h, z if h == 0 else x]
            for j in range(1, SIDE):
                projected = projected + last[k, h, j - 1].astype(jnp.float32)
            one = 0.9 * m1_ref[k, :, cut(h)] + 0.1 * projected
            two = 0.9 * m2_ref[k, :, cut(h)] + 0.1 * projected * projected
            n1_ref[k, :, cut(h)] = one
            n2_ref[k, :, cut(h)] = two
            rounded = (one / (jnp.sqrt(two) + 1e-08)).astype(jnp.bfloat16)
            dirs[k, z, x, :, cut(h)] = rounded
            for j in FIRST:
                dir_first(k, h, j).start()
            value = rounded.astype(jnp.float32)
            square = square + value * value
        return jnp.where(lane == k, jnp.sum(square), 0.0)

    def pass_dirs(ks):
        all_of(group_of(last, ks), 3, dir_recv.at[ks[0] // 2]).wait_recv()
        for h, j in ALL:
            for k in ks:
                dir_second(k, h, j).start()

    def pair_copy(k, tile):
        view = red.at[k, tile_rows(k // 2, tile), :]
        return pltpu.make_async_remote_copy(
            src_ref=view,
            dst_ref=view,
            send_sem=send_sem.at[5],
            recv_sem=pair_recv.at[k // 2],
            device_id=(me, partner),
            device_id_type=MESH,
        )

    def pair_half(ks, recv):
        view = red.at[ks, pl.ds(0, tokens // 2), :]
        return all_of(view, 5, recv, (me, partner))

    def reduce_pair(tile):
        load(0, *streams[0], tile).wait()
        rows = x_buf[held_rows(0, tile), :]
        at = tile_rows(0, tile)
        first = jnp.dot(rows, b_buf[0], preferred_element_type=jnp.float32)
        second = jnp.dot(rows, b_buf[1], preferred_element_type=jnp.float32)
        red[0, at, :] = first.astype(jnp.bfloat16)
        red[1, at, :] = second.astype(jnp.bfloat16)
        for k in range(2):
            pair_copy(k, tile).start()

    def reduce_last(tile):
        load(1, *streams[1], tile).wait()
        start, count = cuts[1][tile]
        half = count * quarter_rows // 2
        upper = pl.ds(start * quarter_rows, half)
        lower = pl.ds(start * quarter_rows + half, half)
        first = jnp.dot(oc_buf[upper, :], b_buf[2], preferred_element_type=jnp.float32)
        second = jnp.dot(oc_buf[lower, :], b_buf[2], preferred_element_type=jnp.float32)
        both = jnp.concatenate([first, second], axis=0)
        red[2, tile_rows(1, tile), :] = both.astype(jnp.bfloat16)
        pair_copy(2, tile).start()

    def fold(left, right):
        return lax.dot_general(
            left, right, (((0,), (0,)), ((), ())), preferred_element_type=jnp.float32
        )

    def project_pair():
        for k in range(2):
            load_all(k).wait()
        pair_half(pl.ds(0, 2), pair_recv.at[0]).wait_recv()
        shape = acc.shape[1:]
        first = fold(red[0], c_buf[0])
        second = fold(red[1], c_buf[1])
        acc[0] = first.reshape(shape)
        acc[1] = second.reshape(shape)
        part[0] = (first * factor).astype(jnp.bfloat16).reshape(shape)
        part[1] = (second * factor).astype(jnp.bfloat16).reshape(shape)

    def project_last():
        load_all(2).wait()
        pair_half(pl.ds(2, 1), pair_recv.at[1]).wait_recv()
        half = tokens // 2
        total = fold(red[2, :half, :], c_buf[2, :half, :])
        total = total + fold(red[2, half:, :], c_buf[2, half:, :])
        acc[2] = total.reshape(acc.shape[1:])
        part[2] = (total * factor).astype(jnp.bfloat16).reshape(acc.shape[1:])

    for tile in range(1, len(cuts[0])):
        load(0, *streams[0], tile).start(priority=1)
    with jax.named_scope("barrier"):
        pl.semaphore_wait(barrier, len(around))
    next_to = [around[0], around[2], around[4], around[5]]
    for place in next_to:
        pl.semaphore_signal(near_sem, inc=1, device_id=place, device_id_type=MESH)
    stage_0()
    with jax.named_scope("compute0"):
        for k in range(2):
            base_copies[k].wait()
        for tile in range(len(cuts[0])):
            reduce_pair(tile)
            if tile == 0:
                base_copies[2].start()
                for later in range(len(cuts[1])):
                    load(1, *streams[1], later).start()
            elif tile == 1:
                for k in range(3):
                    load_all(k).start()
                for copy in firsts[3:]:
                    copy.start()
    with jax.named_scope("compute2"):
        base_copies[2].wait()
        for tile in range(len(cuts[1])):
            reduce_last(tile)
    stage_1()
    with jax.named_scope("project0"):
        project_pair()
        pl.semaphore_wait(near_sem, len(next_to))
        pl.semaphore_signal(
            across_sem, inc=1, device_id=(me, along_y(2)), device_id_type=MESH
        )
        send_parts(0)
        send_parts(1)
    with jax.named_scope("project2"):
        project_last()
        send_parts(2)
    stage_far(1)
    stage_on(0)
    with jax.named_scope("pass0"):
        pl.semaphore_wait(across_sem, 1)
        pass_parts((0, 1))
    with jax.named_scope("pass2"):
        pass_parts((2,))
    stage_far(2)
    for copy in firsts[3:]:
        copy.wait()
    def total_copy(j):
        return pltpu.make_async_remote_copy(
            src_ref=totals.at[0],
            dst_ref=totals.at[j],
            send_sem=send_sem.at[6],
            recv_sem=sum_recv.at[1],
            device_id=(ahead(0, j), mt),
            device_id_type=MESH,
        )

    def sum_copy(j):
        return pltpu.make_async_remote_copy(
            src_ref=sums.at[0],
            dst_ref=sums.at[j],
            send_sem=send_sem.at[7],
            recv_sem=sum_recv.at[0],
            device_id=(ahead(j // groups, 0), lax.rem(mt + j % groups, groups)),
            device_id_type=MESH,
        )

    def sums_arrived():
        return all_of(sums.at[pl.ds(1, SIDE * groups - 1)], 7, sum_recv.at[0])

    def totals_arrived():
        return all_of(totals.at[pl.ds(1, SIDE - 1)], 6, sum_recv.at[1])

    with jax.named_scope("combine0"):
        stage_on(1)
        own_sum = combine((0, 1))
    with jax.named_scope("combine2"):
        sums[0] = own_sum + combine((2,))
    for dz in (2, 1, 3, 0):
        for dt in (4, 5, 3, 2, 6, 7, 1, 0):
            if dz + dt > 0:
                sum_copy(dz * groups + dt).start()
    with jax.named_scope("stage2"):
        stage_3()
        stage_on(2)
    with jax.named_scope("dirs1"):
        pass_dirs((0, 1))
    with jax.named_scope("dirs1b"):
        pass_dirs((2,))
    with jax.named_scope("stage5n"):
        pl.when(core == 1)(lambda: stage_on(3))
    with jax.named_scope("sums"):
        sums_arrived().wait_recv()
        total = sums[0]
        for j in range(1, SIDE * groups):
            total = total + sums[j]
        totals[0] = total
        for j in FIRST:
            total_copy(j).start()

    with jax.named_scope("stage5"):
        pl.when(core == 0)(lambda: stage_on(3))
    with jax.named_scope("dirs2"):
        all_of(got, 4, dir_recv.at[2]).wait_recv()
    with jax.named_scope("totals"):
        totals_arrived().wait_recv()
        for j in range(1, SIDE):
            total = total + totals[j]
        scale = lax.rsqrt(total / entries + 1.0)
        for k in range(3):
            scale_ref[k] = jnp.broadcast_to(scale[:, k : k + 1], scale_ref.shape[1:])
    with jax.named_scope("stage6"):
        w_arrived(6)

    with jax.named_scope("drain"):
        all_of(all_w.at[pl.ds(0, size - 1)], 0, w_recv.at[0]).wait_send()
        all_of(got, 1, dir_recv.at[2]).wait_send()
        all_of(last, 2, dir_recv.at[0]).wait_send()
        all_of(last, 3, dir_recv.at[0]).wait_send()
        all_of(got, 4, dir_recv.at[2]).wait_send()
        pair_half(pl.ds(0, 3), pair_recv.at[0]).wait_send()
        totals_arrived().wait_send()
        sums_arrived().wait_send()


def exchange(size, groups, x, oc, fc, vc, go, bases, fw, vw, ow, m1, m2):
    tokens, width = x.shape
    rank = bases.shape[2]
    rows, columns = fw.shape
    rank_rows = m1.shape[1]
    bf16, f32 = jnp.bfloat16, jnp.float32
    vmem = pl.BlockSpec(memory_space=pltpu.VMEM)
    dma = pltpu.SemaphoreType.DMA
    kernel = functools.partial(
        exchange_kernel,
        size,
        groups,
        float(tokens * size) ** (-0.5),
        float(rank * columns * groups),
    )
    return pl.pallas_call(
        kernel,
        out_shape=(
            pltpu.VMEM((size, 3, rows, columns), bf16),
            pltpu.VMEM((3, SIDE, SIDE, rank_rows, columns), bf16),
            pltpu.VMEM(bases.shape, bf16),
            pltpu.VMEM((3, 8, 512), f32),
            pltpu.VMEM(m1.shape, f32),
            pltpu.VMEM(m2.shape, f32),
            pltpu.VMEM(fw.shape, f32),
            pltpu.VMEM(vw.shape, f32),
            pltpu.VMEM(ow.shape, f32),
        ),
        in_specs=[pl.BlockSpec(memory_space=pltpu.HBM)] * 11,
        out_specs=(vmem,) * 9,
        scratch_shapes=[
            pltpu.VMEM(m1.shape, f32),
            pltpu.VMEM(m2.shape, f32),
            pltpu.VMEM((tokens // 2, width), bf16),
            pltpu.VMEM((tokens // 2, width), bf16),
            pltpu.VMEM((3, tokens, columns), bf16),
            pltpu.VMEM((3, tokens, rank), bf16),
            pltpu.VMEM((3, SIDE, SIDE, rank_rows, columns), f32),
            pltpu.VMEM((3, SIDE, SIDE, rank_rows, columns), bf16),
            pltpu.VMEM((3, 2, SIDE - 1, SIDE, rank_rows, columns // 2), bf16),
            pltpu.VMEM((3, 2, SIDE, rank_rows, columns // 2), f32),
            pltpu.VMEM((3, 2, SIDE, rank_rows, columns // 2), bf16),
            pltpu.VMEM((3, 2, SIDE - 1, rank_rows, columns // 2), bf16),
            pltpu.VMEM((SIDE * groups, 1, 128), f32),
            pltpu.VMEM((SIDE, 1, 128), f32),
            dma((5,)),
            dma((2, 3)),
            dma((3,)),
            dma((3,)),
            dma((2,)),
            dma((8,)),
            dma((7,)),
            dma((2, 2)),
            dma((3,)),
            dma((2,)),
            pltpu.SemaphoreType.REGULAR,
            pltpu.SemaphoreType.REGULAR,
        ],
        compiler_params=pltpu.CompilerParams(
            collective_id=0, has_side_effects=True, vmem_limit_bytes=52 * 1024 * 1024
        ),
    )(x, oc, fc, vc, go, bases, fw, vw, ow, m1, m2)


def finish_kernel(
    scale_ref,
    dirs_ref,
    all_w,
    bases_ref,
    fw_ref,
    vw_ref,
    ow_ref,
    n1_ref,
    n2_ref,
    new_f,
    new_v,
    new_o,
    copy_f,
    copy_v,
    copy_o,
    n1_out,
    n2_out,
    step_f,
    step_v,
    step_o,
    cf_buf,
    cv_buf,
    co_buf,
    down_buf,
    across_buf,
    tile_sem,
    small_sem,
):
    tiles = 8
    rows = cf_buf.shape[0] // tiles
    own = fw_ref.shape[0]
    owners = rows // own

    def put(src, dst, sem):
        pltpu.make_async_copy(src, dst, sem).start()

    put(n1_ref, n1_out, small_sem.at[0])
    put(n2_ref, n2_out, small_sem.at[1])

    def direction(k):
        return dirs_ref[k].reshape(bases_ref.shape[2], down_buf.shape[2])

    def down(at, k):
        step = jnp.dot(bases_ref[k, at, :], direction(k), preferred_element_type=jnp.float32)
        return step * scale_ref[k, 0:1, : step.shape[1]]

    def across(at):
        step = lax.dot_general(
            direction(2),
            bases_ref[2, at, :],
            (((0,), (1,)), ((), ())),
            preferred_element_type=jnp.float32,
        )
        return step * scale_ref[2, 0:1, : step.shape[1]]

    me = pl.ds(pl.multiple_of(lax.axis_index("fs") * own, own), own)
    for k, weight, new, out in ((0, fw_ref, new_f, step_f), (1, vw_ref, new_v, step_v)):
        step = down(me, k)
        down_buf[2 * k] = step
        put(down_buf.at[2 * k], out, small_sem.at[2])
        down_buf[2 * k + 1] = weight[...] - 0.01 * step
        put(down_buf.at[2 * k + 1], new, small_sem.at[2])
    step = across(me)
    across_buf[0] = step
    put(across_buf.at[0], step_o, small_sem.at[3])
    across_buf[1] = ow_ref[...] - 0.01 * step
    put(across_buf.at[1], new_o, small_sem.at[3])

    for tile in range(tiles):
        at = pl.ds(tile * rows, rows)
        owned = pl.ds(tile * owners, owners)
        for k, buf, out in ((0, cf_buf, copy_f), (1, cv_buf, copy_v)):
            old = all_w[owned, k].reshape(rows, cf_buf.shape[1])
            value = old.astype(jnp.float32) - 0.01 * down(at, k)
            buf[at, :] = value.astype(jnp.bfloat16)
            put(buf.at[at, :], out.at[at, :], tile_sem.at[k])
        step = across(at)
        for i in range(owners):
            lanes = pl.ds(tile * rows + i * own, own)
            for j in range(2):
                old = all_w[tile * owners + i, 2, :, j * own : (j + 1) * own]
                value = old.astype(jnp.float32) - 0.01 * step[
                    j * own : (j + 1) * own, i * own : (i + 1) * own
                ]
                co_buf[pl.ds(j * own, own), lanes] = value.astype(jnp.bfloat16)
        put(co_buf.at[:, at], copy_o.at[:, at], tile_sem.at[2])

    for i, buf, out in ((0, cf_buf, copy_f), (1, cv_buf, copy_v), (2, co_buf, copy_o)):
        pltpu.make_async_copy(buf, out, tile_sem.at[i]).wait()
    pltpu.make_async_copy(n1_ref, n1_out, small_sem.at[0]).wait()
    pltpu.make_async_copy(n2_ref, n2_out, small_sem.at[1]).wait()
    pltpu.make_async_copy(down_buf, down_buf, small_sem.at[2]).wait()
    pltpu.make_async_copy(across_buf, across_buf, small_sem.at[3]).wait()


def finish(all_w, dirs, bases, scales, one, two, fw, vw, ow):
    size, _, rows, columns = all_w.shape
    depth = size * rows
    rank = bases.shape[2]
    bf16, f32 = jnp.bfloat16, jnp.float32
    dma = pltpu.SemaphoreType.DMA
    tall = jax.ShapeDtypeStruct((depth, columns), bf16)
    wide = jax.ShapeDtypeStruct((columns, depth), bf16)
    down = jax.ShapeDtypeStruct((rows, columns), f32)
    across = jax.ShapeDtypeStruct((columns, rows), f32)
    small = jax.ShapeDtypeStruct(one.shape, f32)
    return pl.pallas_call(
        finish_kernel,
        out_shape=(down, down, across, tall, tall, wide, small, small, down, down, across),
        in_specs=[pl.BlockSpec(memory_space=pltpu.VMEM)] * 9,
        out_specs=(pl.BlockSpec(memory_space=pltpu.HBM),) * 11,
        scratch_shapes=[
            pltpu.VMEM(tall.shape, bf16),
            pltpu.VMEM(tall.shape, bf16),
            pltpu.VMEM(wide.shape, bf16),
            pltpu.VMEM((4,) + down.shape, f32),
            pltpu.VMEM((2,) + across.shape, f32),
            dma((3,)),
            dma((4,)),
        ],
        compiler_params=pltpu.CompilerParams(vmem_limit_bytes=24 * 1024 * 1024),
        cost_estimate=pl.CostEstimate(
            flops=6 * depth * rank * columns, bytes_accessed=8 * depth * columns, transcendentals=0
        ),
    )(scales, dirs, all_w, bases, fw, vw, ow, one, two)


def on_device(
    normed_input,
    forget_cot,
    value_cot,
    gated_output,
    output_cot,
    forget_weight,
    value_weight,
    out_weight,
    bases,
    first_moment,
    second_moment,
):
    size, groups = lax.axis_size("fs"), lax.axis_size("tp")
    held = exchange(
        size,
        groups,
        normed_input,
        output_cot,
        forget_cot,
        value_cot,
        gated_output,
        bases,
        forget_weight,
        value_weight,
        out_weight,
        first_moment.transpose(1, 0, 2),
        second_moment.transpose(1, 0, 2),
    )
    outs = finish(*held)
    return (
        *outs[:6],
        outs[6].transpose(1, 0, 2),
        outs[7].transpose(1, 0, 2),
        *outs[8:],
    )


def solution(mesh):
    placed = (
        P("fs", None),
        P("fs", "tp"),
        P("fs", "tp"),
        P("fs", "tp"),
        P("fs", None),
        P("fs", "tp"),
        P("fs", "tp"),
        P("tp", "fs"),
        P(),
        P("fs", None, "tp"),
        P("fs", None, "tp"),
    )
    return jax.shard_map(
        on_device,
        mesh=mesh,
        in_specs=placed,
        out_specs=(
            P("fs", "tp"),
            P("fs", "tp"),
            P("tp", "fs"),
            P(None, "tp"),
            P(None, "tp"),
            P("tp", None),
            P("fs", None, "tp"),
            P("fs", None, "tp"),
            P("fs", "tp"),
            P("fs", "tp"),
            P("tp", "fs"),
        ),
        check_vma=False,
    )
```
